32 devices in a mesh: sp: 16 (over z, y, x), tp: 2 (over core).
Axes of the slice: x: 2, y: 2, z: 4, core: 2. Of those that a mesh axis runs over, the one named last changes fastest.
Arguments:
- queries: bfloat16 [8192, 2048], P('sp', 'tp'), may hold values from -6 to 6
- key_rows: bfloat16 [8192, 512], P('sp', 'tp'), may hold values from -6 to 6
- values: bfloat16 [8192, 512], P('sp', 'tp'), may hold values from -6 to 6
- sink_logit: float32 [32], P('tp'), may hold values from 4 to 10
- residual_in: bfloat16 [8192, 2048], P(('sp', 'tp')), may hold values from -6 to 6
- out_weight: bfloat16 [2048, 2048], P('tp'), may hold values from -0.125 to 0.125
- norm_gain: float32 [2048], replicated, may hold values from 0.1 to 1.9
- gate_weight: bfloat16 [2048, 5632], P('sp', 'tp'), may hold values from -0.125 to 0.125
- up_weight: bfloat16 [2048, 5632], P('sp', 'tp'), may hold values from -0.125 to 0.125
- down_weight: bfloat16 [5632, 2048], P('tp', 'sp'), may hold values from -0.078125 to 0.078125
Outputs:
- layer_out: bfloat16 [8192, 2048], P(('sp', 'tp'))
The draws below stay inside these ranges and needn't reach their ends.
All inputs are finite; a program needn't handle non-finite values.
Results may differ from the reference program's by a relative error of at most 0.013.
Values may be sent and summed in bfloat16 or wider, within the bound.
A program may use at most 128 MiB of HBM per device.

```python
import jax
import jax.numpy as jnp
from jax import lax

D = 2048
HEADS = 32
KV_HEADS = 8
HEAD_DIM = 64
FF = 5632
WINDOW = 128
TOK_DEV = 512
TOKENS = 8192
N_TP = 2


def base_draw(key, columns):
    return jnp.clip(1.7 * jax.random.normal(key, (TOKENS, columns), jnp.float32), -6.0, 6.0)


def draw_queries(key, part):
    result = base_draw(jax.random.fold_in(key, 1), HEADS * HEAD_DIM)
    return result.astype(jnp.bfloat16)


def draw_key_rows(key, part):
    result = base_draw(jax.random.fold_in(key, 2), KV_HEADS * HEAD_DIM)
    return result.astype(jnp.bfloat16)


def level_of(stream_key, dims, split, least, high):
    loudness, own = 1.0, jax.random.fold_in(stream_key, 6)
    for dim, shards_of in split:
        steps = jnp.exp(jax.random.uniform(jax.random.fold_in(own, dim), (shards_of,), jnp.float32, least / len(split), high / len(split)))
        loudness = loudness * jnp.repeat(steps, dims[dim] // shards_of).reshape([-1 if axis == dim else 1 for axis in range(len(dims))])
    return loudness


def scatter_about(rng, dims, spread, limit, shards=(), kind=jnp.bfloat16):
    values = jax.random.normal(rng, dims, jnp.float32) * spread
    if len(shards) > 0:
        values = level_of(rng, dims, shards, -0.22, 0.18) * values
    return jnp.clip(values, min=-limit, max=limit).astype(kind)


def setup_inputs(seed: int = 0) -> dict:
    key_list = jax.random.split(jax.random.key(seed), 11)
    return {
        "queries": draw_queries(jax.random.fold_in(key_list[10], 71), 0),
        "key_rows": draw_key_rows(jax.random.fold_in(key_list[10], 71), 0),
        "values": scatter_about(key_list[2], (TOKENS, KV_HEADS * HEAD_DIM), 1.0, 6.0, ((0, 16), (1, 2))),
        "sink_logit": jnp.clip(4.0 + 6.0 * jax.random.uniform(key_list[3], (HEADS,), jnp.float32) ** level_of(key_list[3], (HEADS,), ((0, 2),), -0.2, 0.2), 4.0, 10.0),
        "residual_in": scatter_about(key_list[4], (TOKENS, D), 1.0, 6.0, ((0, 32),)),
        "out_weight": scatter_about(key_list[5], (HEADS * HEAD_DIM, D), (HEADS * HEAD_DIM) ** -0.5, 0.125, ((0, 2),)),
        "norm_gain": jnp.clip(1.0 + 0.18 * jax.random.normal(key_list[6], (D,), jnp.float32), 0.1, 1.9),
        "gate_weight": scatter_about(key_list[7], (D, FF), D ** -0.5, 0.125, ((0, 16), (1, 2))),
        "up_weight": scatter_about(key_list[8], (D, FF), D ** -0.5, 0.125, ((0, 16), (1, 2))),
        "down_weight": scatter_about(key_list[9], (FF, D), FF ** -0.5, 0.078125, ((0, 2), (1, 16))),
    }


def rms_scale(mixed_rows, norm_gain):
    inverse = lax.rsqrt(lax.optimization_barrier(jnp.mean(mixed_rows * mixed_rows, axis=-1, keepdims=True)) + 1e-06)
    return (mixed_rows * inverse * norm_gain).astype(jnp.bfloat16)

def rounded_sum(left, right, parts):
    columns = left.shape[1] // parts
    summed = jnp.zeros((left.shape[0], right.shape[1]), jnp.float32)
    for part_index in range(parts):
        partial_value = jnp.dot(left[:, part_index * columns:(part_index + 1) * columns], right[part_index * columns:(part_index + 1) * columns], preferred_element_type=jnp.float32)
        summed = summed + lax.optimization_barrier(partial_value.astype(jnp.bfloat16)).astype(jnp.float32)
    return summed

def reference(queries, key_rows, values, sink_logit, residual_in, out_weight, norm_gain, gate_weight, up_weight, down_weight):
    group_size = HEADS // KV_HEADS
    score_scale = HEAD_DIM ** (-0.5)
    block_count = TOKENS // WINDOW
    zero_rows = jnp.zeros((WINDOW, KV_HEADS * HEAD_DIM), jnp.bfloat16)
    key_padded = jnp.concatenate([zero_rows, key_rows, zero_rows], axis=0)
    value_padded = jnp.concatenate([zero_rows, values, zero_rows], axis=0)
    sink_grid = sink_logit.astype(jnp.float32).reshape(KV_HEADS, group_size)[:, :, None, None]

    def one_block(block_index):
        start_row = (block_index * WINDOW).astype(jnp.int32)
        query_block = lax.dynamic_slice_in_dim(queries, start_row, WINDOW, 0).astype(jnp.float32)
        query_block = query_block.reshape(WINDOW, KV_HEADS, group_size, HEAD_DIM)
        key_block = lax.dynamic_slice_in_dim(key_padded, start_row, 3 * WINDOW, 0).astype(jnp.float32)
        key_block = key_block.reshape(3 * WINDOW, KV_HEADS, HEAD_DIM)
        value_block = lax.dynamic_slice_in_dim(value_padded, start_row, 3 * WINDOW, 0).astype(jnp.float32)
        value_block = value_block.reshape(3 * WINDOW, KV_HEADS, HEAD_DIM)
        scores = jnp.einsum('qkgd,skd->kgqs', query_block, key_block) * score_scale
        query_pos = start_row + jnp.arange(WINDOW, dtype=jnp.int32)
        key_pos = start_row - WINDOW + jnp.arange(3 * WINDOW, dtype=jnp.int32)
        valid = (jnp.abs(query_pos[:, None] - key_pos[None, :]) <= WINDOW) & (key_pos >= 0)[None, :] & (key_pos < TOKENS)[None, :]
        scores = jnp.where(valid, scores, -1e+30)
        peak = jnp.maximum(lax.optimization_barrier(jnp.max(scores, axis=-1, keepdims=True)), sink_grid)
        weights_raw = jnp.exp(scores - peak)
        denom = lax.optimization_barrier(jnp.sum(weights_raw, axis=-1, keepdims=True)) + jnp.exp(sink_grid - peak)
        probs = lax.optimization_barrier((weights_raw / denom).astype(jnp.bfloat16)).astype(jnp.float32)
        output = jnp.einsum('kgqs,skd->qkgd', probs, value_block).astype(jnp.bfloat16)
        return output.reshape(WINDOW, HEADS * HEAD_DIM)
    attended = lax.map(one_block, jnp.arange(block_count, dtype=jnp.int32)).reshape(TOKENS, HEADS * HEAD_DIM)
    attn_sum = rounded_sum(attended, out_weight, N_TP)
    mixed_rows = residual_in.astype(jnp.float32) + attn_sum

    def feed_forward(mixed_block):
        normed = rms_scale(mixed_block, norm_gain)
        gate_pre = jnp.dot(normed, gate_weight, preferred_element_type=jnp.float32)
        up_pre = jnp.dot(normed, up_weight, preferred_element_type=jnp.float32)
        hidden = (jax.nn.silu(gate_pre) * up_pre).astype(jnp.bfloat16)
        ffn_sum = rounded_sum(hidden, down_weight, N_TP)
        return (mixed_block + ffn_sum).astype(jnp.bfloat16)
    blocked = mixed_rows.reshape(TOKENS // TOK_DEV, TOK_DEV, D)
    return lax.map(feed_forward, blocked).reshape(TOKENS, D)
```

```python
import math

import jax
import jax.numpy as jnp
from jax import lax
from jax.experimental import pallas as pl
from jax.experimental.pallas import tpu as pltpu
from jax.sharding import Mesh
from jax.sharding import PartitionSpec as P

HEAD_DIM = 64
WINDOW = 128


def with_halo(block, sides, width):
    for axis, dim in sides:
        count = math.prod(lax.axis_size(name) for name in axis)
        forward = [(i, i + 1) for i in range(count - 1)]
        backward = [(target, source) for source, target in forward]
        low = lax.ppermute(
            lax.slice_in_dim(block, block.shape[dim] - width, None, axis=dim), axis, forward
        )
        high = lax.ppermute(lax.slice_in_dim(block, 0, width, axis=dim), axis, backward)
        block = jnp.concatenate([low, block, high], axis=dim)
    return block


def rms_scale(mixed_rows, norm_gain):
    inverse = lax.rsqrt(jnp.mean(mixed_rows * mixed_rows, axis=-1, keepdims=True) + 1e-06)
    return (mixed_rows * inverse * norm_gain).astype(jnp.bfloat16)


def attend_window(queries, padded, offset, total_rows, sink_logit, between):
    rows_here = queries.shape[0]
    block_count = rows_here // WINDOW
    heads_here = queries.shape[1] // HEAD_DIM
    kv_here = padded.shape[1] // (2 * HEAD_DIM)
    group_size = heads_here // kv_here
    blocks = padded.reshape(block_count + 2, WINDOW, padded.shape[1])
    banded = jnp.concatenate([blocks[:-2], blocks[1:-1], blocks[2:]], axis=1)
    key_band = banded[:, :, : kv_here * HEAD_DIM].reshape(
        block_count, 3 * WINDOW, kv_here, HEAD_DIM
    )
    value_band = banded[:, :, kv_here * HEAD_DIM :].reshape(
        block_count, 3 * WINDOW, kv_here, HEAD_DIM
    )
    grouped = queries.reshape(block_count, WINDOW, kv_here, group_size, HEAD_DIM)
    scores = jnp.einsum(
        "nqkgd,nskd->nkgqs", grouped, key_band, preferred_element_type=jnp.float32
    ) * HEAD_DIM ** (-0.5)
    scores, moved = lax.optimization_barrier((scores, between))
    block_start = offset + jnp.arange(block_count, dtype=jnp.int32)[:, None] * WINDOW
    query_pos = block_start + jnp.arange(WINDOW, dtype=jnp.int32)[None, :]
    key_pos = block_start - WINDOW + jnp.arange(3 * WINDOW, dtype=jnp.int32)[None, :]
    valid = jnp.abs(query_pos[:, :, None] - key_pos[:, None, :]) <= WINDOW
    valid = valid & ((key_pos >= 0) & (key_pos < total_rows))[:, None, :]
    scores = jnp.where(valid[:, None, None], scores, -1e30)
    sink_grid = sink_logit.reshape(kv_here, group_size)[None, :, :, None, None]
    peak = jnp.maximum(jnp.max(scores, axis=-1, keepdims=True), sink_grid)
    weights_raw = jnp.exp(scores - peak)
    denom = jnp.sum(weights_raw, axis=-1, keepdims=True) + jnp.exp(sink_grid - peak)
    probs = (weights_raw / denom).astype(jnp.bfloat16)
    output = jnp.einsum("nkgqs,nskd->nqkgd", probs, value_band, preferred_element_type=jnp.float32)
    return output.astype(jnp.bfloat16).reshape(rows_here, heads_here * HEAD_DIM), moved


def swap(array, axis, distance):
    count = lax.axis_size(axis)
    return lax.ppermute(array, axis, [(i, i ^ distance) for i in range(count)])


def turn(array, step):
    count = lax.axis_size("o")
    return lax.ppermute(array, "o", [(i, (i + step) % count) for i in range(count)])


def piece(array, index, size, dim):
    return lax.dynamic_slice_in_dim(array, index * size, size, dim)


def shards(
    queries,
    key_rows,
    values,
    sink_logit,
    residual_in,
    out_weight,
    norm_gain,
    gate_weight,
    up_weight,
    down_weight,
):
    rows_here = queries.shape[0]
    tp_count, group = lax.axis_size("tp"), lax.axis_size("q")
    row_share = rows_here // tp_count
    q_index, tp_index = lax.axis_index("q"), lax.axis_index("tp")
    units = gate_weight.shape[1] // group

    joined = jnp.concatenate([key_rows, values], axis=1)
    padded = with_halo(joined, ((("o", "q"), 0),), WINDOW)

    gate_up = jnp.stack([gate_weight, up_weight])
    gate_up_got, down_got = [], []
    for k in range(group):
        part = piece(gate_up, q_index ^ k, units, 2)
        gate_up_got.append(swap(part, "q", k) if k else part)
    for k in range(group):
        part = piece(down_weight, q_index ^ k, units, 0)
        down_got.append(swap(part, "q", k) if k else part)
    depth, width = gate_weight.shape[0], down_weight.shape[1]
    gate_up_mine = jnp.zeros((2, group * depth, units), gate_weight.dtype)
    down_mine = jnp.zeros((units, group * width), down_weight.dtype)
    for k in range(group):
        gate_up_mine = lax.dynamic_update_slice_in_dim(
            gate_up_mine, gate_up_got[k], (q_index ^ k) * depth, 1
        )
        down_mine = lax.dynamic_update_slice_in_dim(
            down_mine, down_got[k], (q_index ^ k) * width, 1
        )
    sp_index = lax.axis_index(("o", "q"))
    total_rows = rows_here * lax.axis_size(("o", "q"))
    mine = (gate_up_mine[0], gate_up_mine[1], down_mine)
    attended, mine = attend_window(
        queries, padded, sp_index * rows_here, total_rows, sink_logit, mine
    )
    outer = lax.axis_size("o")
    pieces = [(0, mine)]
    rings = [(x, x) for x in mine]
    if outer > 2:
        rings = [(turn(x, 1), turn(x, -1)) for x in mine]
        attended, rings[0] = lax.optimization_barrier((attended, rings[0]))

    partial_value = jnp.dot(attended, out_weight, preferred_element_type=jnp.float32).astype(
        jnp.bfloat16
    )
    mixed = residual_in.astype(jnp.float32) + piece(partial_value, tp_index, row_share, 0).astype(
        jnp.float32
    )
    for j in range(1, tp_count):
        sent = piece(partial_value, tp_index ^ j, row_share, 0)
        mixed = mixed + swap(sent, "tp", j).astype(jnp.float32)
    normed = rms_scale(mixed, norm_gain)

    own = normed
    if outer > 2:
        own, rings[1] = lax.optimization_barrier((normed, rings[1]))
        pieces += [(-1, [x for x, _ in rings]), (1, [y for _, y in rings])]
    for distance in range(2, (outer - 1) // 2 + 1):
        rings = [(turn(x, 1), turn(y, -1)) for x, y in rings]
        pieces += [(-distance, [x for x, _ in rings]), (distance, [y for _, y in rings])]
    if outer > 1 and outer % 2 == 0:
        far = []
        for x, y in rings:
            half = x.shape[0] // 2
            far.append(jnp.concatenate([turn(x[:half], 1), turn(y[half:], -1)], axis=0))
        pieces.append((outer // 2, far))
    gate_full = jnp.zeros((outer * group * depth, units), gate_weight.dtype)
    up_full = jnp.zeros((outer * group * depth, units), gate_weight.dtype)
    down_full = jnp.zeros((units, outer * group * width), down_weight.dtype)
    for distance, (gate_part, up_part, down_part) in pieces:
        place = lax.rem(lax.axis_index("o") + distance + outer, outer)
        row = place * group * depth
        gate_full = lax.dynamic_update_slice_in_dim(gate_full, gate_part, row, 0)
        up_full = lax.dynamic_update_slice_in_dim(up_full, up_part, row, 0)
        down_full = lax.dynamic_update_slice_in_dim(down_full, down_part, place * group * width, 1)

    order = [*range(group - 1, 0, -1), 0]
    arrived = {k: swap(normed, "q", k) for k in order if k}
    arrived[0] = own
    result = mixed
    waiting, received = None, []
    for k in order:
        rows = jnp.concatenate(
            [swap(arrived[k], "tp", j) if j else arrived[k] for j in range(tp_count)], axis=0
        )
        gate_pre = jnp.dot(rows, gate_full, preferred_element_type=jnp.float32)
        up_pre = jnp.dot(rows, up_full, preferred_element_type=jnp.float32)
        hidden = (jax.nn.silu(gate_pre) * up_pre).astype(jnp.bfloat16)
        if waiting is not None:
            sent, hidden = lax.optimization_barrier((waiting[1], hidden))
            received.append(swap(sent, "q", waiting[0]))
        if k == 0 and len(received) > 2:
            received[0], hidden = lax.optimization_barrier((received[0], hidden))
        parts = []
        for j in [*range(1, tp_count), 0]:
            if j == k == 0 and len(received) > 2:
                received[1], parts, hidden = lax.optimization_barrier(
                    (received[1], parts, hidden)
                )
            share = hidden[j * row_share : (j + 1) * row_share]
            out = jnp.dot(share, down_full, preferred_element_type=jnp.float32)
            out = out.astype(jnp.bfloat16)
            parts.append(swap(out, "tp", j) if j else out)
        total = sum(part.astype(jnp.float32) for part in parts)
        if k:
            waiting = (k, total.astype(jnp.bfloat16))
        else:
            result = result + total
    for part in received:
        result = result + part.astype(jnp.float32)
    return result.astype(jnp.bfloat16)


MESH = pl.DeviceIdType.MESH
LANES = 128
NT = (((1,), (1,)), ((), ()))


def chunks_of(units):
    step = 2 * LANES
    return [(start, min(step, units - start)) for start in range(0, units, step)]


def fused(
    q_ref, k_ref, v_ref, sink_ref, res_hbm, ow_hbm, gain_ref, w_ref, o_ref,
    khalo, vhalo, exp_k, exp_v, att, ow, psend, precv, mixed,
    tok, wfull, wrelay, hid, dsend, drecv, own, esend, erecv, ssend, srecv,
    local_sem, halo_ss, halo_rs, p_ss, p_rs, w_ss, w_rs, r_ss, r_rs,
    t_ss, t_rs, d_ss, d_rs, e_ss, e_rs, s_ss, s_rs,
):
    f32, bf16 = jnp.float32, jnp.bfloat16
    sp, c = lax.axis_index("sp"), lax.axis_index("tp")
    sp_count = lax.axis_size("sp")
    x, y, z = sp % 2, (sp // 2) % 2, sp // 4
    xn, yn, zn, zs = 1 - x, 1 - y, z + 1 - 2 * (z % 2), 3 - z
    zf = 3 - zn
    zq = (z * (3 - z)) // 2
    rows = q_ref.shape[0]
    half = rows // 2
    units = wfull.shape[2]
    chunks = chunks_of(units)
    width = wfull.shape[3]
    blocks = wfull.shape[0]

    def place(zz, yy, xx):
        return (zz * 2 + yy) * 2 + xx

    partner = (sp, 1 - c)
    to_x, to_y = (place(z, y, xn), c), (place(z, yn, x), c)
    to_z = [None, (place(zn, y, x), c), (place(zs, y, x), c), (place(zf, y, x), c)]
    z_of = [z, zn, zs, zf]

    barrier = pltpu.get_barrier_semaphore()
    for peer in (partner, to_x, to_y, to_z[1], to_z[2], to_z[3]):
        pl.semaphore_signal(barrier, inc=1, device_id=peer, device_id_type=MESH)

    @pl.when(sp > 0)
    def _():
        pl.semaphore_signal(barrier, inc=1, device_id=(sp - 1, c), device_id_type=MESH)

    @pl.when(sp < sp_count - 1)
    def _():
        pl.semaphore_signal(barrier, inc=1, device_id=(sp + 1, c), device_id_type=MESH)

    low_edge, high_edge = jnp.minimum(sp, 1), jnp.minimum(sp_count - 1 - sp, 1)
    pl.semaphore_wait(barrier, 6 + low_edge + high_edge)

    def remote(src, dst, ss, rs, dev):
        return pltpu.make_async_remote_copy(
            src_ref=src, dst_ref=dst, send_sem=ss, recv_sem=rs, device_id=dev, device_id_type=MESH
        )

    sent = []

    def start(copy):
        copy.start()
        sent.append(copy)

    win = khalo.shape[1]

    def halo(side, dev):
        first = rows - win if side == 0 else 0
        for n, (src, dst) in enumerate(((k_ref, khalo), (v_ref, vhalo))):
            m = 2 * side + n
            yield remote(
                src.at[first : first + win], dst.at[side], halo_ss.at[m], halo_rs.at[m], dev
            )

    @pl.when(sp < sp_count - 1)
    def _():
        for copy in halo(0, (sp + 1, c)):
            copy.start()

    @pl.when(sp > 0)
    def _():
        for copy in halo(1, (sp - 1, c)):
            copy.start()

    def role(dz, dx, dy):
        return (dz * 2 + dx) * 2 + dy

    def part(xx, qq, chunk):
        first = pl.multiple_of((xx * 2 + qq) * units + chunk[0], 64)
        return w_ref.at[:, pl.ds(first, chunk[1]), :]

    def slot(b, chunk):
        return wfull.at[b, :, chunk[0] : chunk[0] + chunk[1], :]

    def relay_slot(chunk):
        return wrelay.at[:, chunk[0] : chunk[0] + chunk[1], :]

    mine, from_x = place(z, y, x), place(z, y, xn)
    copies = {}
    for i, ch in enumerate(chunks):
        r = role(0, 1, 0)
        copies["x", i] = remote(part(xn, zq, ch), slot(mine, ch), w_ss.at[r, i], w_rs.at[r, i], to_x)
        copies["r", i] = remote(part(xn, 1 - zq, ch), relay_slot(ch), r_ss.at[i], r_rs.at[i], to_x)
        for dx, b in ((0, mine), (1, from_x)):
            for dz in (1, 2, 3):
                if dx == 0:
                    src = part(x, zq if dz == 2 else 1 - zq, ch)
                else:
                    src = slot(b, ch) if dz == 2 else relay_slot(ch)
                r = role(dz, dx, 0)
                copies["z", dx, dz, i] = remote(
                    src, slot(b, ch), w_ss.at[r, i], w_rs.at[r, i], to_z[dz]
                )
        for dz in range(4):
            for dx in (0, 1):
                b = place(z_of[dz], y, xn if dx else x)
                src = part(x, zq, ch) if dz == dx == 0 else slot(b, ch)
                r = role(dz, dx, 1)
                copies["y", dz, dx, i] = remote(
                    src, slot(b, ch), w_ss.at[r, i], w_rs.at[r, i], to_y
                )

    def wait_weights(dz, dx, dy, i):
        b = place(z_of[dz], yn if dy else y, xn if dx else x)
        dst = slot(b, chunks[i])
        r = role(dz, dx, dy)
        dev = to_y if dy else to_z[dz] if dz else to_x
        remote(dst, dst, w_ss.at[r, i], w_rs.at[r, i], dev).wait_recv()

    for i in range(len(chunks)):
        for dz in (2, 3, 1):
            start(copies["z", 0, dz, i])
        start(copies["x", i])
        start(copies["r", i])
        start(copies["y", 0, 0, i])

    def x_relay(i):
        wait_weights(0, 1, 0, i)
        remote(relay_slot(chunks[i]), relay_slot(chunks[i]), r_ss.at[i], r_rs.at[i], to_x).wait_recv()
        for dz in (2, 3, 1):
            start(copies["z", 1, dz, i])
        start(copies["y", 0, 1, i])

    def y_relay(dz, dx, i):
        wait_weights(dz, dx, 0, i)
        start(copies["y", dz, dx, i])

    load_ow = pltpu.make_async_copy(ow_hbm, ow, local_sem.at[0])
    load_ow.start()
    own_weights = pltpu.make_async_copy(
        w_ref.at[:, pl.ds(pl.multiple_of((x * 2 + zq) * units, 64), units), :],
        wfull.at[mine], local_sem.at[1],
    )
    own_weights.start()
    load_res = pltpu.make_async_copy(res_hbm, dsend.at[0], local_sem.at[2])
    load_res.start()

    kv_here = k_ref.shape[1] // HEAD_DIM
    heads_here = q_ref.shape[1] // HEAD_DIM
    pairs = heads_here // kv_here // 2

    def spread(src, dst, first):
        count = src.shape[0]
        low = lax.broadcasted_iota(jnp.int32, (count, LANES), 1) < HEAD_DIM
        for j in range(kv_here // 2):
            t = src[:, j * LANES : (j + 1) * LANES].astype(f32)
            r = pltpu.roll(t, HEAD_DIM, 1)
            zero = jnp.zeros_like(t)
            window = slice(first, first + count)
            dst[2 * j, 0, window, :] = jnp.where(low, t, zero).astype(bf16)
            dst[2 * j, 1, window, :] = jnp.where(low, zero, r).astype(bf16)
            dst[2 * j + 1, 0, window, :] = jnp.where(low, r, zero).astype(bf16)
            dst[2 * j + 1, 1, window, :] = jnp.where(low, zero, t).astype(bf16)

    spread(k_ref, exp_k, win)
    spread(v_ref, exp_v, win)

    @pl.when(sp > 0)
    def _():
        for copy in halo(0, (sp - 1, c)):
            copy.wait_recv()

    @pl.when(sp == 0)
    def _():
        khalo[0] = jnp.zeros_like(khalo[0])
        vhalo[0] = jnp.zeros_like(vhalo[0])

    @pl.when(sp < sp_count - 1)
    def _():
        for copy in halo(1, (sp + 1, c)):
            copy.wait_recv()

    @pl.when(sp == sp_count - 1)
    def _():
        khalo[1] = jnp.zeros_like(khalo[1])
        vhalo[1] = jnp.zeros_like(vhalo[1])

    for side, first in ((0, 0), (1, rows + win)):
        spread(khalo.at[side], exp_k, first)
        spread(vhalo.at[side], exp_v, first)

    total_rows = rows * sp_count

    def attend(blk):
        base = pl.multiple_of(blk * win, win)
        stack = (pairs * win, 3 * win)
        i = lax.broadcasted_iota(jnp.int32, stack, 0) % win
        j = lax.broadcasted_iota(jnp.int32, stack, 1)
        key = sp * rows + base - win + j
        valid = (j >= i) & (j <= i + 2 * win) & (key >= 0) & (key < total_rows)
        which = lax.broadcasted_iota(jnp.int32, (pairs * win, 1), 0) // win
        for g in range(kv_here):
            q2 = jnp.concatenate(
                [
                    q_ref[pl.ds(base, win), (g * pairs + p) * LANES : (g * pairs + p + 1) * LANES]
                    for p in range(pairs)
                ],
                axis=0,
            )
            out = None
            for side in range(2):
                kw = exp_k[g, side, pl.ds(base, 3 * win), :]
                scores = lax.dot_general(q2, kw, NT, preferred_element_type=f32) * HEAD_DIM**-0.5
                scores = jnp.where(valid, scores, -1e30)
                sink = jnp.zeros((pairs * win, 1), f32)
                for p in range(pairs):
                    sink = jnp.where(which == p, sink_ref[(g * pairs + p) * 2 + side], sink)
                peak = jnp.maximum(jnp.max(scores, axis=-1, keepdims=True), sink)
                weight = jnp.exp(scores - peak)
                denom = jnp.sum(weight, axis=-1, keepdims=True) + jnp.exp(sink - peak)
                probs = (weight * (1.0 / denom)).astype(bf16)
                vw = exp_v[g, side, pl.ds(base, 3 * win), :]
                got = jnp.dot(probs, vw, preferred_element_type=f32)
                out = got if out is None else out + got
            for p in range(pairs):
                att[pl.ds(base, win), (g * pairs + p) * LANES : (g * pairs + p + 1) * LANES] = out[
                    p * win : (p + 1) * win
                ].astype(bf16)

    def attend_step(blk, carry):
        attend(blk)

        @pl.when(blk == 1)
        def _():
            x_relay(0)

        return carry

    lax.fori_loop(0, rows // win, attend_step, 0)

    depth = mixed.shape[1]
    tile = 4 * LANES
    load_ow.wait()
    other = pl.multiple_of((1 - c) * half, half)
    here = pl.multiple_of(c * half, half)
    for n in range(0, depth, tile):
        psend[:, n : n + tile] = jnp.dot(
            att[pl.ds(other, half), :], ow[:, n : n + tile], preferred_element_type=f32
        ).astype(bf16)
    swap_p = remote(psend, precv, p_ss.at[0], p_rs.at[0], partner)
    start(swap_p)
    x_relay(1)
    load_res.wait()
    for n in range(0, depth, tile):
        partial_out = jnp.dot(
            att[pl.ds(here, half), :], ow[:, n : n + tile], preferred_element_type=f32
        )
        mixed[:, n : n + tile] = dsend[0, :, n : n + tile].astype(f32) + partial_out.astype(
            bf16
        ).astype(f32)
    swap_p.wait_recv()
    step = 64
    for m in range(0, half, step):
        part_mixed = mixed[m : m + step, :] + precv[m : m + step, :].astype(f32)
        mixed[m : m + step, :] = part_mixed
        inverse = lax.rsqrt(jnp.mean(part_mixed * part_mixed, axis=-1, keepdims=True) + 1e-06)
        tok[0, 0, m : m + step, :] = (part_mixed * inverse * gain_ref[...]).astype(bf16)

    def tok_copy(n, src, dst, dev):
        return remote(tok.at[src[0], src[1]], tok.at[dst[0], dst[1]], t_ss.at[n], t_rs.at[n], dev)

    t_x = tok_copy(0, (0, 0), (1, 0), to_x)
    t_z = tok_copy(1, (0, 0), (2, 0), to_z[1])
    t_d = tok_copy(2, (2, 0), (3, 0), to_x)
    t_p = [tok_copy(3 + g, (g, 0), (g, 1), partner) for g in range(4)]
    start(t_x)
    start(t_z)
    start(t_p[0])
    x_relay(2)

    pairs_of = [(b, b + 1) for b in range(0, blocks, 2)]

    def weights_t(m, ch):
        lo, n = ch
        return jnp.concatenate([wfull[b, m, lo : lo + n, :] for b in range(blocks)], axis=1)

    def gate_up(g, i):
        lo, n = chunks[i]

        def body(cc, carry):
            t = tok[g, cc]
            gate = lax.dot_general(t, weights_t(0, chunks[i]), NT, preferred_element_type=f32)
            upv = lax.dot_general(t, weights_t(1, chunks[i]), NT, preferred_element_type=f32)
            hid[g, cc, :, lo : lo + n] = (gate / (1.0 + jnp.exp(-gate)) * upv).astype(bf16)
            return carry

        lax.fori_loop(0, 2, body, 0)

    def project(g, cc, store):
        per = tile // width
        for n in range(0, blocks, per):
            wd = jnp.concatenate([wfull[b, 2] for b in range(n, n + per)], axis=1)
            store(
                slice(n * width, (n + per) * width),
                jnp.dot(hid[g, cc], wd, preferred_element_type=f32),
            )

    def ready(i):
        for dz in range(4):
            for dx in range(2):
                wait_weights(dz, dx, 1, i)

    def relays(i, order):
        for dz, dx in order:
            y_relay(dz, dx, i)

    order = [(1, 0), (2, 0), (1, 1), (2, 1), (3, 0), (3, 1)]
    own_weights.wait()
    relays(0, order)
    ready(0)
    t_p[0].wait_recv()
    gate_up(0, 0)
    relays(1, order[:2])
    t_x.wait_recv()
    start(t_p[1])
    t_z.wait_recv()
    start(t_p[2])
    start(t_d)
    t_p[1].wait_recv()
    gate_up(1, 0)
    relays(1, order[2:4])
    t_p[2].wait_recv()
    gate_up(2, 0)
    relays(1, order[4:])
    ready(1)
    gate_up(0, 1)
    gate_up(1, 1)
    relays(2, order[:2])
    gate_up(2, 1)
    relays(2, order[2:4])
    t_d.wait_recv()
    start(t_p[3])
    t_p[3].wait_recv()
    gate_up(3, 0)
    gate_up(3, 1)
    relays(2, order[4:])
    ready(2)

    def to_partner(g):
        return remote(dsend.at[g], drecv.at[g], d_ss.at[g], d_rs.at[g], partner)

    def send_partner(g):
        def store(cols, value):
            dsend[g, :, cols] = value.astype(bf16)

        project(g, 1, store)
        start(to_partner(g))

    def keep(g, n):
        def store(cols, value):
            own[n, :, cols] = value

        project(g, 0, store)

    quarter = half // 2
    e_x = remote(esend.at[0], erecv.at[0], e_ss.at[0], e_rs.at[0], to_x)
    e_z = remote(esend.at[1], erecv.at[1], e_ss.at[1], e_rs.at[1], to_z[1])

    def out_copy(n, h, dev):
        window = slice(h * quarter, (h + 1) * quarter)
        return remote(
            ssend.at[n, window], srecv.at[n, window], s_ss.at[n, h], s_rs.at[n, h], dev
        )

    out_x = [out_copy(0, h, to_x) for h in range(2)]
    out_z = [out_copy(1, h, to_z[1]) for h in range(2)]

    gate_up(3, 2)
    send_partner(3)
    keep(3, 0)
    gate_up(1, 2)
    to_partner(3).wait_recv()
    for h, copy in ((0, e_x), (1, e_z)):
        window = slice(h * quarter, (h + 1) * quarter)
        esend[h] = (own[0, window, :] + drecv[3, window, :].astype(f32)).astype(bf16)
        start(copy)
    send_partner(1)
    keep(1, 1)
    gate_up(2, 2)
    to_partner(1).wait_recv()
    low, high = slice(0, quarter), slice(quarter, half)
    ssend[0, low, :] = (own[1, low, :] + drecv[1, low, :].astype(f32)).astype(bf16)
    start(out_x[0])
    send_partner(2)
    keep(2, 0)
    gate_up(0, 2)
    to_partner(2).wait_recv()
    ssend[1, high, :] = (own[0, high, :] + drecv[2, high, :].astype(f32)).astype(bf16)
    start(out_z[1])
    send_partner(0)

    def add_mixed(cols, value):
        mixed[:, cols] = mixed[:, cols] + value

    project(0, 0, add_mixed)
    e_z.wait_recv()
    ssend[0, high, :] = (
        own[1, high, :] + drecv[1, high, :].astype(f32) + erecv[1].astype(f32)
    ).astype(bf16)
    start(out_x[1])
    e_x.wait_recv()
    ssend[1, low, :] = (
        own[0, low, :] + drecv[2, low, :].astype(f32) + erecv[0].astype(f32)
    ).astype(bf16)
    start(out_z[0])
    to_partner(0).wait_recv()
    mixed[...] = mixed[...] + drecv[0].astype(f32)
    out_x[0].wait_recv()
    out_z[1].wait_recv()
    out_x[1].wait_recv()
    out_z[0].wait_recv()
    o_ref[...] = (mixed[...] + srecv[0].astype(f32) + srecv[1].astype(f32)).astype(bf16)

    for copy in sent:
        copy.wait_send()

    @pl.when(sp < sp_count - 1)
    def _():
        for copy in halo(0, (sp + 1, c)):
            copy.wait_send()

    @pl.when(sp > 0)
    def _():
        for copy in halo(1, (sp - 1, c)):
            copy.wait_send()


def fused_shards(
    queries, key_rows, values, sink_logit, residual_in, out_weight, norm_gain,
    gate_weight, up_weight, down_weight,
):
    bf16, f32 = jnp.bfloat16, jnp.float32
    rows, depth = queries.shape[0], residual_in.shape[1]
    half = residual_in.shape[0]
    blocks = lax.axis_size("sp")
    kv = key_rows.shape[1]
    kv_here = kv // HEAD_DIM
    width = down_weight.shape[1]
    units = down_weight.shape[0] // 4
    count = len(chunks_of(units))
    weights = jnp.stack([gate_weight.T, up_weight.T, down_weight])
    vmem = pl.BlockSpec(memory_space=pltpu.VMEM)
    smem = pl.BlockSpec(memory_space=pltpu.SMEM)
    hbm = pl.BlockSpec(memory_space=pl.ANY)
    dma = pltpu.SemaphoreType.DMA
    scratch = [
        pltpu.VMEM((2, WINDOW, kv), bf16),
        pltpu.VMEM((2, WINDOW, kv), bf16),
        pltpu.VMEM((kv_here, 2, rows + 2 * WINDOW, LANES), bf16),
        pltpu.VMEM((kv_here, 2, rows + 2 * WINDOW, LANES), bf16),
        pltpu.VMEM(queries.shape, bf16),
        pltpu.VMEM(out_weight.shape, bf16),
        pltpu.VMEM((half, depth), bf16),
        pltpu.VMEM((half, depth), bf16),
        pltpu.VMEM((half, depth), f32),
        pltpu.VMEM((4, 2, half, depth), bf16),
        pltpu.VMEM((blocks, 3, units, width), bf16),
        pltpu.VMEM((3, units, width), bf16),
        pltpu.VMEM((4, 2, half, units), bf16),
        pltpu.VMEM((4, half, depth), bf16),
        pltpu.VMEM((4, half, depth), bf16),
        pltpu.VMEM((2, half, depth), f32),
        pltpu.VMEM((2, half // 2, depth), bf16),
        pltpu.VMEM((2, half // 2, depth), bf16),
        pltpu.VMEM((2, half, depth), bf16),
        pltpu.VMEM((2, half, depth), bf16),
        dma((3,)), dma((4,)), dma((4,)), dma((1,)), dma((1,)),
        dma((16, count)), dma((16, count)), dma((count,)), dma((count,)),
        dma((7,)), dma((7,)), dma((4,)), dma((4,)), dma((2,)), dma((2,)),
        dma((2, 2)), dma((2, 2)),
    ]
    return pl.pallas_call(
        fused,
        out_shape=jax.ShapeDtypeStruct(residual_in.shape, bf16),
        in_specs=[vmem, vmem, vmem, smem, hbm, hbm, vmem, vmem],
        out_specs=vmem,
        scratch_shapes=scratch,
        compiler_params=pltpu.CompilerParams(
            collective_id=0, has_side_effects=True, vmem_limit_bytes=63 * 1024 * 1024
        ),
    )(
        queries, key_rows, values, sink_logit, residual_in, out_weight,
        norm_gain.reshape(1, depth), weights,
    )


def solution(mesh):
    sp_count, tp_count = mesh.shape["sp"], mesh.shape["tp"]
    group = math.gcd(sp_count, 4)
    if tp_count == 2 and sp_count == 4 * group:
        return jax.shard_map(
            fused_shards,
            mesh=mesh,
            in_specs=(
                P("sp", "tp"),
                P("sp", "tp"),
                P("sp", "tp"),
                P("tp"),
                P(("sp", "tp"), None),
                P("tp", None),
                P(),
                P("sp", "tp"),
                P("sp", "tp"),
                P("tp", "sp"),
            ),
            out_specs=P(("sp", "tp"), None),
            check_vma=False,
        )
    fine = Mesh(mesh.devices.reshape(sp_count // group, group, tp_count), ("o", "q", "tp"))
    sp = ("o", "q")
    return jax.shard_map(
        shards,
        mesh=fine,
        in_specs=(
            P(sp, "tp"),
            P(sp, "tp"),
            P(sp, "tp"),
            P("tp"),
            P(("o", "q", "tp"), None),
            P("tp", None),
            P(),
            P(sp, "tp"),
            P(sp, "tp"),
            P("tp", sp),
        ),
        out_specs=P(("o", "q", "tp"), None),
        check_vma=False,
    )
```

```python
import math

import jax
import jax.numpy as jnp
from jax import lax
from jax.experimental import pallas as pl
from jax.experimental.pallas import tpu as pltpu
from jax.sharding import Mesh
from jax.sharding import PartitionSpec as P

HEAD_DIM = 64
WINDOW = 128


def with_halo(block, sides, width):
    for axis, dim in sides:
        count = math.prod(lax.axis_size(name) for name in axis)
        forward = [(i, i + 1) for i in range(count - 1)]
        backward = [(target, source) for source, target in forward]
        low = lax.ppermute(
            lax.slice_in_dim(block, block.shape[dim] - width, None, axis=dim), axis, forward
        )
        high = lax.ppermute(lax.slice_in_dim(block, 0, width, axis=dim), axis, backward)
        block = jnp.concatenate([low, block, high], axis=dim)
    return block


def rms_scale(mixed_rows, norm_gain):
    inverse = lax.rsqrt(jnp.mean(mixed_rows * mixed_rows, axis=-1, keepdims=True) + 1e-06)
    return (mixed_rows * inverse * norm_gain).astype(jnp.bfloat16)


def attend_window(queries, padded, offset, total_rows, sink_logit, between):
    rows_here = queries.shape[0]
    block_count = rows_here // WINDOW
    heads_here = queries.shape[1] // HEAD_DIM
    kv_here = padded.shape[1] // (2 * HEAD_DIM)
    group_size = heads_here // kv_here
    blocks = padded.reshape(block_count + 2, WINDOW, padded.shape[1])
    banded = jnp.concatenate([blocks[:-2], blocks[1:-1], blocks[2:]], axis=1)
    key_band = banded[:, :, : kv_here * HEAD_DIM].reshape(
        block_count, 3 * WINDOW, kv_here, HEAD_DIM
    )
    value_band = banded[:, :, kv_here * HEAD_DIM :].reshape(
        block_count, 3 * WINDOW, kv_here, HEAD_DIM
    )
    grouped = queries.reshape(block_count, WINDOW, kv_here, group_size, HEAD_DIM)
    scores = jnp.einsum(
        "nqkgd,nskd->nkgqs", grouped, key_band, preferred_element_type=jnp.float32
    ) * HEAD_DIM ** (-0.5)
    scores, moved = lax.optimization_barrier((scores, between))
    block_start = offset + jnp.arange(block_count, dtype=jnp.int32)[:, None] * WINDOW
    query_pos = block_start + jnp.arange(WINDOW, dtype=jnp.int32)[None, :]
    key_pos = block_start - WINDOW + jnp.arange(3 * WINDOW, dtype=jnp.int32)[None, :]
    valid = jnp.abs(query_pos[:, :, None] - key_pos[:, None, :]) <= WINDOW
    valid = valid & ((key_pos >= 0) & (key_pos < total_rows))[:, None, :]
    scores = jnp.where(valid[:, None, None], scores, -1e30)
    sink_grid = sink_logit.reshape(kv_here, group_size)[None, :, :, None, None]
    peak = jnp.maximum(jnp.max(scores, axis=-1, keepdims=True), sink_grid)
    weights_raw = jnp.exp(scores - peak)
    denom = jnp.sum(weights_raw, axis=-1, keepdims=True) + jnp.exp(sink_grid - peak)
    probs = (weights_raw / denom).astype(jnp.bfloat16)
    output = jnp.einsum("nkgqs,nskd->nqkgd", probs, value_band, preferred_element_type=jnp.float32)
    return output.astype(jnp.bfloat16).reshape(rows_here, heads_here * HEAD_DIM), moved


def swap(array, axis, distance):
    count = lax.axis_size(axis)
    return lax.ppermute(array, axis, [(i, i ^ distance) for i in range(count)])


def turn(array, step):
    count = lax.axis_size("o")
    return lax.ppermute(array, "o", [(i, (i + step) % count) for i in range(count)])


def piece(array, index, size, dim):
    return lax.dynamic_slice_in_dim(array, index * size, size, dim)


def shards(
    queries,
    key_rows,
    values,
    sink_logit,
    residual_in,
    out_weight,
    norm_gain,
    gate_weight,
    up_weight,
    down_weight,
):
    rows_here = queries.shape[0]
    tp_count, group = lax.axis_size("tp"), lax.axis_size("q")
    row_share = rows_here // tp_count
    q_index, tp_index = lax.axis_index("q"), lax.axis_index("tp")
    units = gate_weight.shape[1] // group

    joined = jnp.concatenate([key_rows, values], axis=1)
    padded = with_halo(joined, ((("o", "q"), 0),), WINDOW)

    gate_up = jnp.stack([gate_weight, up_weight])
    gate_up_got, down_got = [], []
    for k in range(group):
        part = piece(gate_up, q_index ^ k, units, 2)
        gate_up_got.append(swap(part, "q", k) if k else part)
    for k in range(group):
        part = piece(down_weight, q_index ^ k, units, 0)
        down_got.append(swap(part, "q", k) if k else part)
    depth, width = gate_weight.shape[0], down_weight.shape[1]
    gate_up_mine = jnp.zeros((2, group * depth, units), gate_weight.dtype)
    down_mine = jnp.zeros((units, group * width), down_weight.dtype)
    for k in range(group):
        gate_up_mine = lax.dynamic_update_slice_in_dim(
            gate_up_mine, gate_up_got[k], (q_index ^ k) * depth, 1
        )
        down_mine = lax.dynamic_update_slice_in_dim(
            down_mine, down_got[k], (q_index ^ k) * width, 1
        )
    sp_index = lax.axis_index(("o", "q"))
    total_rows = rows_here * lax.axis_size(("o", "q"))
    mine = (gate_up_mine[0], gate_up_mine[1], down_mine)
    attended, mine = attend_window(
        queries, padded, sp_index * rows_here, total_rows, sink_logit, mine
    )
    outer = lax.axis_size("o")
    pieces = [(0, mine)]
    rings = [(x, x) for x in mine]
    if outer > 2:
        rings = [(turn(x, 1), turn(x, -1)) for x in mine]
        attended, rings[0] = lax.optimization_barrier((attended, rings[0]))

    partial_value = jnp.dot(attended, out_weight, preferred_element_type=jnp.float32).astype(
        jnp.bfloat16
    )
    mixed = residual_in.astype(jnp.float32) + piece(partial_value, tp_index, row_share, 0).astype(
        jnp.float32
    )
    for j in range(1, tp_count):
        sent = piece(partial_value, tp_index ^ j, row_share, 0)
        mixed = mixed + swap(sent, "tp", j).astype(jnp.float32)
    normed = rms_scale(mixed, norm_gain)

    own = normed
    if outer > 2:
        own, rings[1] = lax.optimization_barrier((normed, rings[1]))
        pieces += [(-1, [x for x, _ in rings]), (1, [y for _, y in rings])]
    for distance in range(2, (outer - 1) // 2 + 1):
        rings = [(turn(x, 1), turn(y, -1)) for x, y in rings]
        pieces += [(-distance, [x for x, _ in rings]), (distance, [y for _, y in rings])]
    if outer > 1 and outer % 2 == 0:
        far = []
        for x, y in rings:
            half = x.shape[0] // 2
            far.append(jnp.concatenate([turn(x[:half], 1), turn(y[half:], -1)], axis=0))
        pieces.append((outer // 2, far))
    gate_full = jnp.zeros((outer * group * depth, units), gate_weight.dtype)
    up_full = jnp.zeros((outer * group * depth, units), gate_weight.dtype)
    down_full = jnp.zeros((units, outer * group * width), down_weight.dtype)
    for distance, (gate_part, up_part, down_part) in pieces:
        place = lax.rem(lax.axis_index("o") + distance + outer, outer)
        row = place * group * depth
        gate_full = lax.dynamic_update_slice_in_dim(gate_full, gate_part, row, 0)
        up_full = lax.dynamic_update_slice_in_dim(up_full, up_part, row, 0)
        down_full = lax.dynamic_update_slice_in_dim(down_full, down_part, place * group * width, 1)

    order = [*range(group - 1, 0, -1), 0]
    arrived = {k: swap(normed, "q", k) for k in order if k}
    arrived[0] = own
    result = mixed
    waiting, received = None, []
    for k in order:
        rows = jnp.concatenate(
            [swap(arrived[k], "tp", j) if j else arrived[k] for j in range(tp_count)], axis=0
        )
        gate_pre = jnp.dot(rows, gate_full, preferred_element_type=jnp.float32)
        up_pre = jnp.dot(rows, up_full, preferred_element_type=jnp.float32)
        hidden = (jax.nn.silu(gate_pre) * up_pre).astype(jnp.bfloat16)
        if waiting is not None:
            sent, hidden = lax.optimization_barrier((waiting[1], hidden))
            received.append(swap(sent, "q", waiting[0]))
        if k == 0 and len(received) > 2:
            received[0], hidden = lax.optimization_barrier((received[0], hidden))
        parts = []
        for j in [*range(1, tp_count), 0]:
            if j == k == 0 and len(received) > 2:
                received[1], parts, hidden = lax.optimization_barrier(
                    (received[1], parts, hidden)
                )
            share = hidden[j * row_share : (j + 1) * row_share]
            out = jnp.dot(share, down_full, preferred_element_type=jnp.float32)
            out = out.astype(jnp.bfloat16)
            parts.append(swap(out, "tp", j) if j else out)
        total = sum(part.astype(jnp.float32) for part in parts)
        if k:
            waiting = (k, total.astype(jnp.bfloat16))
        else:
            result = result + total
    for part in received:
        result = result + part.astype(jnp.float32)
    return result.astype(jnp.bfloat16)


MESH = pl.DeviceIdType.MESH
LANES = 128
NT = (((1,), (1,)), ((), ()))


def spans_of(units):
    step = 2 * LANES
    return [(start, min(step, units - start)) for start in range(0, units, step)]


def chunks_of(units):
    *full, (start, size) = spans_of(units)
    first = min(size, LANES)
    return [*full, (start, first)] + [(start + first, size - first)] * (size > first)


def fused(
    q_hbm, k_ref, v_ref, sink_ref, res_hbm, ow_hbm, gain_ref, gate_ref, up_ref, down_hbm, o_ref,
    w_ref, q_ref, khalo, vhalo, exp_k, exp_v, att, ow, psend, precv, mixed,
    tok, wfull, wrelay, hid, dsend, drecv, own, esend, erecv, ssend, srecv,
    local_sem, halo_ss, halo_rs, p_ss, p_rs, w_ss, w_rs, r_ss, r_rs,
    t_ss, t_rs, d_ss, d_rs, e_ss, e_rs, s_ss, s_rs,
):
    f32, bf16 = jnp.float32, jnp.bfloat16
    sp, c = lax.axis_index("sp"), lax.axis_index("tp")
    sp_count = lax.axis_size("sp")
    x, y, z = sp % 2, (sp // 2) % 2, sp // 4
    xn, yn, zn, zs = 1 - x, 1 - y, z + 1 - 2 * (z % 2), 3 - z
    zf = 3 - zn
    zq = (z * (3 - z)) // 2
    rows = q_ref.shape[0]
    half = rows // 2
    units = wfull.shape[2]
    chunks, spans = chunks_of(units), spans_of(units)
    width = wfull.shape[3]
    blocks = wfull.shape[0]

    def place(zz, yy, xx):
        return (zz * 2 + yy) * 2 + xx

    partner = (sp, 1 - c)
    to_x, to_y = (place(z, y, xn), c), (place(z, yn, x), c)
    to_z = [None, (place(zn, y, x), c), (place(zs, y, x), c), (place(zf, y, x), c)]

    barrier = pltpu.get_barrier_semaphore()
    for peer in (partner, to_x, to_y, to_z[1], to_z[2], to_z[3]):
        pl.semaphore_signal(barrier, inc=1, device_id=peer, device_id_type=MESH)

    @pl.when(sp > 0)
    def _():
        pl.semaphore_signal(barrier, inc=1, device_id=(sp - 1, c), device_id_type=MESH)

    @pl.when(sp < sp_count - 1)
    def _():
        pl.semaphore_signal(barrier, inc=1, device_id=(sp + 1, c), device_id_type=MESH)

    load_down = pltpu.make_async_copy(down_hbm, w_ref.at[2], local_sem.at[3])
    load_down.start()
    load_q = pltpu.make_async_copy(q_hbm, q_ref, local_sem.at[4])
    load_q.start()
    with jax.named_scope("transpose"):
        for first in range(0, gate_ref.shape[1], LANES):
            window = slice(first, first + LANES)
            w_ref[0, window, :] = gate_ref[:, window].T
            w_ref[1, window, :] = up_ref[:, window].T

    low_edge, high_edge = jnp.minimum(sp, 1), jnp.minimum(sp_count - 1 - sp, 1)
    with jax.named_scope("enter"):
        pl.semaphore_wait(barrier, 6 + low_edge + high_edge)
        load_down.wait()

    def remote(src, dst, ss, rs, dev):
        return pltpu.make_async_remote_copy(
            src_ref=src, dst_ref=dst, send_sem=ss, recv_sem=rs, device_id=dev, device_id_type=MESH
        )

    def arrived(copy, name):
        with jax.named_scope(name):
            copy.wait_recv()

    sent = []

    def start(copy):
        copy.start()
        sent.append(copy)

    win = khalo.shape[1]

    def halo(side, dev):
        first = rows - win if side == 0 else 0
        for n, (src, dst) in enumerate(((k_ref, khalo), (v_ref, vhalo))):
            m = 2 * side + n
            yield remote(
                src.at[first : first + win], dst.at[side], halo_ss.at[m], halo_rs.at[m], dev
            )

    @pl.when(sp < sp_count - 1)
    def _():
        for copy in halo(0, (sp + 1, c)):
            copy.start()

    @pl.when(sp > 0)
    def _():
        for copy in halo(1, (sp - 1, c)):
            copy.start()

    def role(dz, dx, dy):
        return (dz * 2 + dx) * 2 + dy

    def part(xx, qq, chunk):
        first = pl.multiple_of((xx * 2 + qq) * units + chunk[0], 64)
        return w_ref.at[:, pl.ds(first, chunk[1]), :]

    def slot(b, chunk):
        return wfull.at[b, :, chunk[0] : chunk[0] + chunk[1], :]

    def relay_slot(chunk):
        return wrelay.at[:, chunk[0] : chunk[0] + chunk[1], :]

    mine, from_x = place(z, y, x), place(z, y, xn)
    copies = {}
    for i, ch in enumerate(chunks):
        r = role(0, 1, 0)
        copies["x", i] = remote(part(xn, zq, ch), slot(mine, ch), w_ss.at[r, i], w_rs.at[r, i], to_x)
        copies["r", i] = remote(part(xn, 1 - zq, ch), relay_slot(ch), r_ss.at[i], r_rs.at[i], to_x)
        for dx, b in ((0, mine), (1, from_x)):
            for dz in (1, 2, 3):
                if dx == 0:
                    src = part(x, zq if dz == 2 else 1 - zq, ch)
                else:
                    src = slot(b, ch) if dz == 2 else relay_slot(ch)
                r = role(dz, dx, 0)
                copies["z", dx, dz, i] = remote(
                    src, slot(b, ch), w_ss.at[r, i], w_rs.at[r, i], to_z[dz]
                )

    z_of = [z, zn, zs, zf]
    OWN, NEAR, SAME, FAR = range(4)
    count = len(chunks)

    def wait_relay(i):
        window = relay_slot(chunks[i])
        remote(window, window, r_ss.at[i], r_rs.at[i], to_x).wait_recv()

    def block_of(dz, dx, dy):
        return place(z_of[dz], yn if dy else y, xn if dx else x)

    def wait_weights(dz, dx, dy, i):
        dst = slot(block_of(dz, dx, dy), chunks[i])
        r = role(dz, dx, dy)
        dev = to_y if dy else to_z[dz] if dz else to_x
        remote(dst, dst, w_ss.at[r, i], w_rs.at[r, i], dev).wait_recv()

    def to_y_copy(dz, dx, i):
        b = block_of(dz, dx, 0)
        src = part(x, zq, chunks[i]) if dz == dx == 0 else slot(b, chunks[i])
        r = role(dz, dx, 1)
        return remote(src, slot(b, chunks[i]), w_ss.at[r, i], w_rs.at[r, i], to_y)

    to_y_copies = {
        (dz, dx, i): to_y_copy(dz, dx, i)
        for dz in range(4) for dx in range(2) for i in range(count)
    }

    def y_relay(dz, dx, i):
        with jax.named_scope(f"y#dz={dz}#dx={dx}#i={i}"):
            wait_weights(dz, dx, 0, i)
            to_y_copies[dz, dx, i].start()

    def by_plane(step, outer, inner):
        @pl.when(zq == 0)
        def _():
            for key in outer:
                step(*key)

        @pl.when(zq == 1)
        def _():
            for key in inner:
                step(*key)

    def serve(outer, inner):
        by_plane(y_relay, outer, inner)

    def z_send(dz, dx, i):
        copies["z", dx, dz, i].start()

    def x_send(i):
        copies["x", i].start()
        copies["r", i].start()

    with jax.named_scope("issue"):
        for dz in (SAME, FAR, NEAR):
            z_send(dz, 0, 0)
        x_send(0)
        for i in range(count):
            to_y_copies[0, 0, i].start()

    load_ow = pltpu.make_async_copy(ow_hbm, ow, local_sem.at[0])
    load_ow.start()
    own_weights = pltpu.make_async_copy(
        w_ref.at[:, pl.ds(pl.multiple_of((x * 2 + zq) * units, 64), units), :],
        wfull.at[mine], local_sem.at[1],
    )
    own_weights.start()
    load_res = pltpu.make_async_copy(res_hbm, dsend.at[0], local_sem.at[2])
    load_res.start()

    kv_here = k_ref.shape[1] // HEAD_DIM
    heads_here = q_ref.shape[1] // HEAD_DIM
    pairs = heads_here // kv_here // 2

    def spread(src, dst, first):
        count = src.shape[0]
        low = lax.broadcasted_iota(jnp.int32, (count, LANES), 1) < HEAD_DIM
        for j in range(kv_here // 2):
            t = src[:, j * LANES : (j + 1) * LANES].astype(f32)
            r = pltpu.roll(t, HEAD_DIM, 1)
            zero = jnp.zeros_like(t)
            window = slice(first, first + count)
            dst[2 * j, 0, window, :] = jnp.where(low, t, zero).astype(bf16)
            dst[2 * j, 1, window, :] = jnp.where(low, zero, r).astype(bf16)
            dst[2 * j + 1, 0, window, :] = jnp.where(low, r, zero).astype(bf16)
            dst[2 * j + 1, 1, window, :] = jnp.where(low, zero, t).astype(bf16)

    with jax.named_scope("spread"):
        spread(k_ref, exp_k, win)
        spread(v_ref, exp_v, win)

    def take_halo():
        @pl.when(sp > 0)
        def _():
            for copy in halo(0, (sp - 1, c)):
                arrived(copy, "halo")

        @pl.when(sp == 0)
        def _():
            khalo[0] = jnp.zeros_like(khalo[0])
            vhalo[0] = jnp.zeros_like(vhalo[0])

        @pl.when(sp < sp_count - 1)
        def _():
            for copy in halo(1, (sp + 1, c)):
                arrived(copy, "halo")

        @pl.when(sp == sp_count - 1)
        def _():
            khalo[1] = jnp.zeros_like(khalo[1])
            vhalo[1] = jnp.zeros_like(vhalo[1])

        for side, first in ((0, 0), (1, rows + win)):
            spread(khalo.at[side], exp_k, first)
            spread(vhalo.at[side], exp_v, first)

    total_rows = rows * sp_count

    def attend(blk):
        base = pl.multiple_of(blk * win, win)
        stack = (pairs * win, 3 * win)
        i = lax.broadcasted_iota(jnp.int32, stack, 0) % win
        j = lax.broadcasted_iota(jnp.int32, stack, 1)
        key = sp * rows + base - win + j
        valid = (j >= i) & (j <= i + 2 * win) & (key >= 0) & (key < total_rows)
        which = lax.broadcasted_iota(jnp.int32, (pairs * win, 1), 0) // win
        for g in range(kv_here):
            q2 = jnp.concatenate(
                [
                    q_ref[pl.ds(base, win), (g * pairs + p) * LANES : (g * pairs + p + 1) * LANES]
                    for p in range(pairs)
                ],
                axis=0,
            )
            out = None
            for side in range(2):
                kw = exp_k[g, side, pl.ds(base, 3 * win), :]
                scores = lax.dot_general(q2, kw, NT, preferred_element_type=f32) * HEAD_DIM**-0.5
                scores = jnp.where(valid, scores, -1e30)
                sink = jnp.zeros((pairs * win, 1), f32)
                for p in range(pairs):
                    sink = jnp.where(which == p, sink_ref[(g * pairs + p) * 2 + side], sink)
                peak = jnp.maximum(jnp.max(scores, axis=-1, keepdims=True), sink)
                weight = jnp.exp(scores - peak)
                denom = jnp.sum(weight, axis=-1, keepdims=True) + jnp.exp(sink - peak)
                probs = (weight * (1.0 / denom)).astype(bf16)
                vw = exp_v[g, side, pl.ds(base, 3 * win), :]
                got = jnp.dot(probs, vw, preferred_element_type=f32)
                out = got if out is None else out + got
            for p in range(pairs):
                att[pl.ds(base, win), (g * pairs + p) * LANES : (g * pairs + p + 1) * LANES] = out[
                    p * win : (p + 1) * win
                ].astype(bf16)

    def attend_step(n, carry):
        inner = rows // win - 2

        @pl.when(n == inner)
        def _():
            take_halo()

        attend(jnp.where(n < inner, n + 1, (n - inner) * (inner + 1)))

        @pl.when(n == 1)
        def _():
            x_send(1)
            by_plane(z_send, [], [(dz, 0, 1) for dz in (SAME, FAR, NEAR)])

        @pl.when(n == inner)
        def _():
            y_relay(OWN, 1, 0)
            wait_relay(0)
            for dz in (SAME, FAR, NEAR):
                z_send(dz, 1, 0)

        @pl.when(n == inner + 1)
        def _():
            for i in range(2, count):
                x_send(i)

        return carry

    with jax.named_scope("attention"):
        load_q.wait()
        lax.fori_loop(0, rows // win, attend_step, 0)

    depth = mixed.shape[1]
    tile = 4 * LANES
    load_ow.wait()
    other = pl.multiple_of((1 - c) * half, half)
    here = pl.multiple_of(c * half, half)
    for n in range(0, depth, tile):
        psend[:, n : n + tile] = jnp.dot(
            att[pl.ds(other, half), :], ow[:, n : n + tile], preferred_element_type=f32
        ).astype(bf16)
    swap_p = remote(psend, precv, p_ss.at[0], p_rs.at[0], partner)
    start(swap_p)
    load_res.wait()
    for n in range(0, depth, tile):
        partial_out = jnp.dot(
            att[pl.ds(here, half), :], ow[:, n : n + tile], preferred_element_type=f32
        )
        mixed[:, n : n + tile] = dsend[0, :, n : n + tile].astype(f32) + partial_out.astype(
            bf16
        ).astype(f32)
    arrived(swap_p, "swap")
    step = 64
    for m in range(0, half, step):
        part_mixed = mixed[m : m + step, :] + precv[m : m + step, :].astype(f32)
        mixed[m : m + step, :] = part_mixed
        inverse = lax.rsqrt(jnp.mean(part_mixed * part_mixed, axis=-1, keepdims=True) + 1e-06)
        tok[0, 0, m : m + step, :] = (part_mixed * inverse * gain_ref[...]).astype(bf16)

    def tok_copy(n, src, dst, dev):
        return remote(tok.at[src[0], src[1]], tok.at[dst[0], dst[1]], t_ss.at[n], t_rs.at[n], dev)

    t_x = tok_copy(0, (0, 0), (1, 0), to_x)
    t_z = tok_copy(1, (0, 0), (2, 0), to_z[1])
    t_d = tok_copy(2, (2, 0), (3, 0), to_x)
    t_p = [tok_copy(3 + g, (g, 0), (g, 1), partner) for g in range(4)]
    start(t_z)
    start(t_x)
    start(t_p[0])
    by_plane(z_send, [(dz, 0, 1) for dz in (SAME, FAR, NEAR)], [])
    serve([(NEAR, 0, 0), (SAME, 0, 0)], [(SAME, 0, 0)])
    for i in range(1, count):
        y_relay(OWN, 1, i)
        wait_relay(i)
        if i > 1:
            for dz in (SAME, FAR, NEAR):
                z_send(dz, 0, i)
        for dz in (SAME, FAR, NEAR):
            z_send(dz, 1, i)

    def weights_t(m, ch):
        lo, n = ch
        return jnp.concatenate([wfull[b, m, lo : lo + n, :] for b in range(blocks)], axis=1)

    def gate_up_rows(g, cc, i):
        lo, n = spans[i]
        t = tok[g, cc]
        gate = lax.dot_general(t, weights_t(0, spans[i]), NT, preferred_element_type=f32)
        upv = lax.dot_general(t, weights_t(1, spans[i]), NT, preferred_element_type=f32)
        hid[g, cc, :, lo : lo + n] = (gate / (1.0 + jnp.exp(-gate)) * upv).astype(bf16)

    def gate_up(g, i):
        def body(cc, carry):
            gate_up_rows(g, cc, i)
            return carry

        with jax.named_scope(f"gu#g={g}#i={i}"):
            lax.fori_loop(0, 2, body, 0)

    def project(g, cc, store):
        per = tile // width
        for n in range(0, blocks, per):
            wd = jnp.concatenate([wfull[b, 2] for b in range(n, n + per)], axis=1)
            store(
                slice(n * width, (n + per) * width),
                jnp.dot(hid[g, cc], wd, preferred_element_type=f32),
            )

    def ready(i):
        with jax.named_scope(f"ready#i={i}"):
            for dz in range(4):
                for dx in range(2):
                    wait_weights(dz, dx, 1, i)

    own_weights.wait()
    serve([(FAR, 0, 0)], [(FAR, 0, 0), (NEAR, 0, 0)])
    serve([(NEAR, 1, 0), (SAME, 1, 0), (FAR, 1, 0)], [(SAME, 1, 0), (FAR, 1, 0), (NEAR, 1, 0)])
    serve([(FAR, 0, 1), (NEAR, 0, 1)], [(SAME, 0, 1)])
    arrived(t_x, "t_x")
    start(t_p[1])
    ready(0)
    arrived(t_p[0], "t_p0")
    gate_up(0, 0)
    serve([(FAR, 1, 1)], [(SAME, 1, 1)])
    arrived(t_p[1], "t_p1")
    gate_up(1, 0)
    serve([(SAME, 0, 1)], [(FAR, 0, 1)])
    arrived(t_z, "t_z")
    start(t_d)
    start(t_p[2])
    serve([(FAR, 0, 2)], [(NEAR, 0, 1), (SAME, 0, 2)])
    arrived(t_p[2], "t_p2")
    gate_up(2, 0)
    serve([(NEAR, 1, 1), (SAME, 1, 1)], [(FAR, 1, 1), (NEAR, 1, 1)])
    serve([(FAR, 1, 2), (NEAR, 0, 2)], [(SAME, 1, 2)])
    serve([(SAME, 0, 2), (NEAR, 1, 2)], [(FAR, 0, 2), (NEAR, 0, 2)])
    ready(1)
    gate_up(0, 1)
    serve([(SAME, 1, 2), (FAR, 0, 3)], [(FAR, 1, 2), (SAME, 0, 3)])
    gate_up(1, 1)
    serve([(NEAR, 0, 3), (SAME, 0, 3)], [(NEAR, 1, 2), (FAR, 0, 3)])
    gate_up(2, 1)
    serve([(FAR, 1, 3), (NEAR, 1, 3), (SAME, 1, 3)], [(SAME, 1, 3), (NEAR, 0, 3), (FAR, 1, 3), (NEAR, 1, 3)])
    arrived(t_d, "t_d")
    start(t_p[3])
    for i in range(2, count):
        ready(i)

    quarter = half // 2
    last = len(spans) - 1
    parts = [slice(0, quarter), slice(quarter, half)]

    def to_partner(g, h):
        return remote(
            dsend.at[g, parts[h]], drecv.at[g, parts[h]], d_ss.at[g, h], d_rs.at[g, h], partner
        )

    def send_partner(g, order):
        def store(cols, value):
            dsend[g, :, cols] = value.astype(bf16)

        with jax.named_scope(f"send#g={g}"):
            gate_up_rows(g, 1, last)
            project(g, 1, store)
            for h in order:
                start(to_partner(g, h))

    def keep(g, n):
        def store(cols, value):
            own[n, :, cols] = value

        with jax.named_scope(f"keep#g={g}"):
            gate_up_rows(g, 0, last)
            project(g, 0, store)

    def summed(g, n, h):
        arrived(to_partner(g, h), f"partner#g={g}")
        return own[n, parts[h], :] + drecv[g, parts[h], :].astype(f32)

    e_x = remote(esend.at[0], erecv.at[0], e_ss.at[0], e_rs.at[0], to_x)
    e_z = remote(esend.at[1], erecv.at[1], e_ss.at[1], e_rs.at[1], to_z[1])

    def out_copy(n, h, dev):
        return remote(
            ssend.at[n, parts[h]], srecv.at[n, parts[h]], s_ss.at[n, h], s_rs.at[n, h], dev
        )

    out_x = [out_copy(0, h, to_x) for h in range(2)]
    out_z = [out_copy(1, h, to_z[1]) for h in range(2)]

    send_partner(1, (0, 1))
    keep(1, 1)
    ssend[0, parts[0], :] = summed(1, 1, 0).astype(bf16)
    start(out_x[0])
    send_partner(2, (1, 0))
    keep(2, 0)
    ssend[1, parts[1], :] = summed(2, 0, 1).astype(bf16)
    start(out_z[1])
    arrived(t_p[3], "t_p3")
    for i in range(last):
        gate_up(3, i)
    send_partner(3, (0, 1))
    keep(3, 2)
    esend[0] = summed(3, 2, 0).astype(bf16)
    start(e_x)
    esend[1] = summed(3, 2, 1).astype(bf16)
    start(e_z)
    send_partner(0, (0, 1))

    def add_mixed(cols, value):
        mixed[:, cols] = mixed[:, cols] + value

    gate_up_rows(0, 0, last)
    project(0, 0, add_mixed)
    own[1, parts[1], :] = summed(1, 1, 1)
    own[0, parts[0], :] = summed(2, 0, 0)
    for h in range(2):
        arrived(to_partner(0, h), "partner0")
    mixed[...] = mixed[...] + drecv[0].astype(f32)

    def pass_on(along_x):
        if along_x:
            arrived(e_z, "e_z")
            ssend[0, parts[1], :] = (own[1, parts[1], :] + erecv[1].astype(f32)).astype(bf16)
            out_x[1].start()
        else:
            arrived(e_x, "e_x")
            ssend[1, parts[0], :] = (own[0, parts[0], :] + erecv[0].astype(f32)).astype(bf16)
            out_z[0].start()

    by_plane(pass_on, [(True,), (False,)], [(False,), (True,)])
    sent.extend((out_x[1], out_z[0]))
    arrived(out_x[0], "out_x0")
    mixed[parts[0], :] = mixed[parts[0], :] + srecv[0, parts[0], :].astype(f32)
    arrived(out_z[1], "out_z1")
    mixed[parts[1], :] = mixed[parts[1], :] + srecv[1, parts[1], :].astype(f32)
    arrived(out_x[1], "out_x1")
    o_ref[parts[1], :] = (mixed[parts[1], :] + srecv[0, parts[1], :].astype(f32)).astype(bf16)
    arrived(out_z[0], "out_z0")
    o_ref[parts[0], :] = (mixed[parts[0], :] + srecv[1, parts[0], :].astype(f32)).astype(bf16)

    for copy in [*sent, *copies.values(), *to_y_copies.values()]:
        copy.wait_send()

    @pl.when(sp < sp_count - 1)
    def _():
        for copy in halo(0, (sp + 1, c)):
            copy.wait_send()

    @pl.when(sp > 0)
    def _():
        for copy in halo(1, (sp - 1, c)):
            copy.wait_send()


def fused_shards(
    queries, key_rows, values, sink_logit, residual_in, out_weight, norm_gain,
    gate_weight, up_weight, down_weight,
):
    bf16, f32 = jnp.bfloat16, jnp.float32
    rows, depth = queries.shape[0], residual_in.shape[1]
    half = residual_in.shape[0]
    blocks = lax.axis_size("sp")
    kv = key_rows.shape[1]
    kv_here = kv // HEAD_DIM
    width = down_weight.shape[1]
    units = down_weight.shape[0] // 4
    count = len(chunks_of(units))
    vmem = pl.BlockSpec(memory_space=pltpu.VMEM)
    smem = pl.BlockSpec(memory_space=pltpu.SMEM)
    hbm = pl.BlockSpec(memory_space=pl.ANY)
    dma = pltpu.SemaphoreType.DMA
    scratch = [
        pltpu.VMEM((3, down_weight.shape[0], width), bf16),
        pltpu.VMEM(queries.shape, bf16),
        pltpu.VMEM((2, WINDOW, kv), bf16),
        pltpu.VMEM((2, WINDOW, kv), bf16),
        pltpu.VMEM((kv_here, 2, rows + 2 * WINDOW, LANES), bf16),
        pltpu.VMEM((kv_here, 2, rows + 2 * WINDOW, LANES), bf16),
        pltpu.VMEM(queries.shape, bf16),
        pltpu.VMEM(out_weight.shape, bf16),
        pltpu.VMEM((half, depth), bf16),
        pltpu.VMEM((half, depth), bf16),
        pltpu.VMEM((half, depth), f32),
        pltpu.VMEM((4, 2, half, depth), bf16),
        pltpu.VMEM((blocks, 3, units, width), bf16),
        pltpu.VMEM((3, units, width), bf16),
        pltpu.VMEM((4, 2, half, units), bf16),
        pltpu.VMEM((4, half, depth), bf16),
        pltpu.VMEM((4, half, depth), bf16),
        pltpu.VMEM((3, half, depth), f32),
        pltpu.VMEM((2, half // 2, depth), bf16),
        pltpu.VMEM((2, half // 2, depth), bf16),
        pltpu.VMEM((2, half, depth), bf16),
        pltpu.VMEM((2, half, depth), bf16),
        dma((5,)), dma((4,)), dma((4,)), dma((1,)), dma((1,)),
        dma((16, count)), dma((16, count)), dma((count,)), dma((count,)),
        dma((7,)), dma((7,)), dma((4, 2)), dma((4, 2)), dma((2,)), dma((2,)),
        dma((2, 2)), dma((2, 2)),
    ]
    return pl.pallas_call(
        fused,
        out_shape=jax.ShapeDtypeStruct(residual_in.shape, bf16),
        in_specs=[hbm, vmem, vmem, smem, hbm, hbm, vmem, vmem, vmem, hbm],
        out_specs=vmem,
        scratch_shapes=scratch,
        compiler_params=pltpu.CompilerParams(
            collective_id=0, has_side_effects=True, vmem_limit_bytes=63 * 1024 * 1024
        ),
    )(
        queries, key_rows, values, sink_logit, residual_in, out_weight,
        norm_gain.reshape(1, depth), gate_weight, up_weight, down_weight,
    )


def solution(mesh):
    sp_count, tp_count = mesh.shape["sp"], mesh.shape["tp"]
    group = math.gcd(sp_count, 4)
    if tp_count == 2 and sp_count == 4 * group:
        return jax.shard_map(
            fused_shards,
            mesh=mesh,
            in_specs=(
                P("sp", "tp"),
                P("sp", "tp"),
                P("sp", "tp"),
                P("tp"),
                P(("sp", "tp"), None),
                P("tp", None),
                P(),
                P("sp", "tp"),
                P("sp", "tp"),
                P("tp", "sp"),
            ),
            out_specs=P(("sp", "tp"), None),
            check_vma=False,
        )
    fine = Mesh(mesh.devices.reshape(sp_count // group, group, tp_count), ("o", "q", "tp"))
    sp = ("o", "q")
    return jax.shard_map(
        shards,
        mesh=fine,
        in_specs=(
            P(sp, "tp"),
            P(sp, "tp"),
            P(sp, "tp"),
            P("tp"),
            P(("o", "q", "tp"), None),
            P("tp", None),
            P(),
            P(sp, "tp"),
            P(sp, "tp"),
            P("tp", sp),
        ),
        out_specs=P(("o", "q", "tp"), None),
        check_vma=False,
    )
```

```python
import math

import jax
import jax.numpy as jnp
from jax import lax
from jax.experimental import pallas as pl
from jax.experimental.pallas import tpu as pltpu
from jax.sharding import Mesh
from jax.sharding import PartitionSpec as P

HEAD_DIM = 64
WINDOW = 128


def with_halo(block, sides, width):
    for axis, dim in sides:
        count = math.prod(lax.axis_size(name) for name in axis)
        forward = [(i, i + 1) for i in range(count - 1)]
        backward = [(target, source) for source, target in forward]
        low = lax.ppermute(
            lax.slice_in_dim(block, block.shape[dim] - width, None, axis=dim), axis, forward
        )
        high = lax.ppermute(lax.slice_in_dim(block, 0, width, axis=dim), axis, backward)
        block = jnp.concatenate([low, block, high], axis=dim)
    return block


def rms_scale(mixed_rows, norm_gain):
    inverse = lax.rsqrt(jnp.mean(mixed_rows * mixed_rows, axis=-1, keepdims=True) + 1e-06)
    return (mixed_rows * inverse * norm_gain).astype(jnp.bfloat16)


def attend_window(queries, padded, offset, total_rows, sink_logit, between):
    rows_here = queries.shape[0]
    block_count = rows_here // WINDOW
    heads_here = queries.shape[1] // HEAD_DIM
    kv_here = padded.shape[1] // (2 * HEAD_DIM)
    group_size = heads_here // kv_here
    blocks = padded.reshape(block_count + 2, WINDOW, padded.shape[1])
    banded = jnp.concatenate([blocks[:-2], blocks[1:-1], blocks[2:]], axis=1)
    key_band = banded[:, :, : kv_here * HEAD_DIM].reshape(
        block_count, 3 * WINDOW, kv_here, HEAD_DIM
    )
    value_band = banded[:, :, kv_here * HEAD_DIM :].reshape(
        block_count, 3 * WINDOW, kv_here, HEAD_DIM
    )
    grouped = queries.reshape(block_count, WINDOW, kv_here, group_size, HEAD_DIM)
    scores = jnp.einsum(
        "nqkgd,nskd->nkgqs", grouped, key_band, preferred_element_type=jnp.float32
    ) * HEAD_DIM ** (-0.5)
    scores, moved = lax.optimization_barrier((scores, between))
    block_start = offset + jnp.arange(block_count, dtype=jnp.int32)[:, None] * WINDOW
    query_pos = block_start + jnp.arange(WINDOW, dtype=jnp.int32)[None, :]
    key_pos = block_start - WINDOW + jnp.arange(3 * WINDOW, dtype=jnp.int32)[None, :]
    valid = jnp.abs(query_pos[:, :, None] - key_pos[:, None, :]) <= WINDOW
    valid = valid & ((key_pos >= 0) & (key_pos < total_rows))[:, None, :]
    scores = jnp.where(valid[:, None, None], scores, -1e30)
    sink_grid = sink_logit.reshape(kv_here, group_size)[None, :, :, None, None]
    peak = jnp.maximum(jnp.max(scores, axis=-1, keepdims=True), sink_grid)
    weights_raw = jnp.exp(scores - peak)
    denom = jnp.sum(weights_raw, axis=-1, keepdims=True) + jnp.exp(sink_grid - peak)
    probs = (weights_raw / denom).astype(jnp.bfloat16)
    output = jnp.einsum("nkgqs,nskd->nqkgd", probs, value_band, preferred_element_type=jnp.float32)
    return output.astype(jnp.bfloat16).reshape(rows_here, heads_here * HEAD_DIM), moved


def swap(array, axis, distance):
    count = lax.axis_size(axis)
    return lax.ppermute(array, axis, [(i, i ^ distance) for i in range(count)])


def turn(array, step):
    count = lax.axis_size("o")
    return lax.ppermute(array, "o", [(i, (i + step) % count) for i in range(count)])


def piece(array, index, size, dim):
    return lax.dynamic_slice_in_dim(array, index * size, size, dim)


def shards(
    queries,
    key_rows,
    values,
    sink_logit,
    residual_in,
    out_weight,
    norm_gain,
    gate_weight,
    up_weight,
    down_weight,
):
    rows_here = queries.shape[0]
    tp_count, group = lax.axis_size("tp"), lax.axis_size("q")
    row_share = rows_here // tp_count
    q_index, tp_index = lax.axis_index("q"), lax.axis_index("tp")
    units = gate_weight.shape[1] // group

    joined = jnp.concatenate([key_rows, values], axis=1)
    padded = with_halo(joined, ((("o", "q"), 0),), WINDOW)

    gate_up = jnp.stack([gate_weight, up_weight])
    gate_up_got, down_got = [], []
    for k in range(group):
        part = piece(gate_up, q_index ^ k, units, 2)
        gate_up_got.append(swap(part, "q", k) if k else part)
    for k in range(group):
        part = piece(down_weight, q_index ^ k, units, 0)
        down_got.append(swap(part, "q", k) if k else part)
    depth, width = gate_weight.shape[0], down_weight.shape[1]
    gate_up_mine = jnp.zeros((2, group * depth, units), gate_weight.dtype)
    down_mine = jnp.zeros((units, group * width), down_weight.dtype)
    for k in range(group):
        gate_up_mine = lax.dynamic_update_slice_in_dim(
            gate_up_mine, gate_up_got[k], (q_index ^ k) * depth, 1
        )
        down_mine = lax.dynamic_update_slice_in_dim(
            down_mine, down_got[k], (q_index ^ k) * width, 1
        )
    sp_index = lax.axis_index(("o", "q"))
    total_rows = rows_here * lax.axis_size(("o", "q"))
    mine = (gate_up_mine[0], gate_up_mine[1], down_mine)
    attended, mine = attend_window(
        queries, padded, sp_index * rows_here, total_rows, sink_logit, mine
    )
    outer = lax.axis_size("o")
    pieces = [(0, mine)]
    rings = [(x, x) for x in mine]
    if outer > 2:
        rings = [(turn(x, 1), turn(x, -1)) for x in mine]
        attended, rings[0] = lax.optimization_barrier((attended, rings[0]))

    partial_value = jnp.dot(attended, out_weight, preferred_element_type=jnp.float32).astype(
        jnp.bfloat16
    )
    mixed = residual_in.astype(jnp.float32) + piece(partial_value, tp_index, row_share, 0).astype(
        jnp.float32
    )
    for j in range(1, tp_count):
        sent = piece(partial_value, tp_index ^ j, row_share, 0)
        mixed = mixed + swap(sent, "tp", j).astype(jnp.float32)
    normed = rms_scale(mixed, norm_gain)

    own = normed
    if outer > 2:
        own, rings[1] = lax.optimization_barrier((normed, rings[1]))
        pieces += [(-1, [x for x, _ in rings]), (1, [y for _, y in rings])]
    for distance in range(2, (outer - 1) // 2 + 1):
        rings = [(turn(x, 1), turn(y, -1)) for x, y in rings]
        pieces += [(-distance, [x for x, _ in rings]), (distance, [y for _, y in rings])]
    if outer > 1 and outer % 2 == 0:
        far = []
        for x, y in rings:
            half = x.shape[0] // 2
            far.append(jnp.concatenate([turn(x[:half], 1), turn(y[half:], -1)], axis=0))
        pieces.append((outer // 2, far))
    gate_full = jnp.zeros((outer * group * depth, units), gate_weight.dtype)
    up_full = jnp.zeros((outer * group * depth, units), gate_weight.dtype)
    down_full = jnp.zeros((units, outer * group * width), down_weight.dtype)
    for distance, (gate_part, up_part, down_part) in pieces:
        place = lax.rem(lax.axis_index("o") + distance + outer, outer)
        row = place * group * depth
        gate_full = lax.dynamic_update_slice_in_dim(gate_full, gate_part, row, 0)
        up_full = lax.dynamic_update_slice_in_dim(up_full, up_part, row, 0)
        down_full = lax.dynamic_update_slice_in_dim(down_full, down_part, place * group * width, 1)

    order = [*range(group - 1, 0, -1), 0]
    arrived = {k: swap(normed, "q", k) for k in order if k}
    arrived[0] = own
    result = mixed
    waiting, received = None, []
    for k in order:
        rows = jnp.concatenate(
            [swap(arrived[k], "tp", j) if j else arrived[k] for j in range(tp_count)], axis=0
        )
        gate_pre = jnp.dot(rows, gate_full, preferred_element_type=jnp.float32)
        up_pre = jnp.dot(rows, up_full, preferred_element_type=jnp.float32)
        hidden = (jax.nn.silu(gate_pre) * up_pre).astype(jnp.bfloat16)
        if waiting is not None:
            sent, hidden = lax.optimization_barrier((waiting[1], hidden))
            received.append(swap(sent, "q", waiting[0]))
        if k == 0 and len(received) > 2:
            received[0], hidden = lax.optimization_barrier((received[0], hidden))
        parts = []
        for j in [*range(1, tp_count), 0]:
            if j == k == 0 and len(received) > 2:
                received[1], parts, hidden = lax.optimization_barrier(
                    (received[1], parts, hidden)
                )
            share = hidden[j * row_share : (j + 1) * row_share]
            out = jnp.dot(share, down_full, preferred_element_type=jnp.float32)
            out = out.astype(jnp.bfloat16)
            parts.append(swap(out, "tp", j) if j else out)
        total = sum(part.astype(jnp.float32) for part in parts)
        if k:
            waiting = (k, total.astype(jnp.bfloat16))
        else:
            result = result + total
    for part in received:
        result = result + part.astype(jnp.float32)
    return result.astype(jnp.bfloat16)


MESH = pl.DeviceIdType.MESH
LANES = 128
NT = (((1,), (1,)), ((), ()))


def spans_of(units):
    step = 2 * LANES
    return [(start, min(step, units - start)) for start in range(0, units, step)]


def chunks_of(units):
    *full, (start, size) = spans_of(units)
    first = min(size, LANES)
    return [*full, (start, first)] + [(start + first, size - first)] * (size > first)


def fused(
    q_hbm, k_hbm, v_hbm, sink_ref, res_hbm, ow_hbm, gain_hbm, gate_hbm, up_hbm, down_hbm, o_hbm,
    k_ref, v_ref, gain_ref, gate_ref, up_ref, w_ref, q_ref, khalo, vhalo, exp_k, exp_v, att, ow, psend, precv, mixed,
    tok, wfull, wrelay, hid, dsend, drecv, own, esend, erecv, ssend, srecv,
    local_sem, halo_ss, halo_rs, p_ss, p_rs, w_ss, w_rs, r_ss, r_rs,
    t_ss, t_rs, d_ss, d_rs, e_ss, e_rs, s_ss, s_rs,
):
    f32, bf16 = jnp.float32, jnp.bfloat16
    sp, c = lax.axis_index("sp"), lax.axis_index("tp")
    sp_count = lax.axis_size("sp")
    x, y, z = sp % 2, (sp // 2) % 2, sp // 4
    xn, yn, zn, zs = 1 - x, 1 - y, z + 1 - 2 * (z % 2), 3 - z
    zf = 3 - zn
    zq = (z * (3 - z)) // 2
    rows = q_ref.shape[0]
    half = rows // 2
    units = wfull.shape[2]
    chunks, spans = chunks_of(units), spans_of(units)
    width = wfull.shape[3]
    blocks = wfull.shape[0]

    def place(zz, yy, xx):
        return (zz * 2 + yy) * 2 + xx

    partner = (sp, 1 - c)
    to_x, to_y = (place(z, y, xn), c), (place(z, yn, x), c)
    to_z = [None, (place(zn, y, x), c), (place(zs, y, x), c), (place(zf, y, x), c)]

    barrier = pltpu.get_barrier_semaphore()
    for peer in (partner, to_x, to_y, to_z[1], to_z[2], to_z[3]):
        pl.semaphore_signal(barrier, inc=1, device_id=peer, device_id_type=MESH)

    @pl.when(sp > 0)
    def _():
        pl.semaphore_signal(barrier, inc=1, device_id=(sp - 1, c), device_id_type=MESH)

    @pl.when(sp < sp_count - 1)
    def _():
        pl.semaphore_signal(barrier, inc=1, device_id=(sp + 1, c), device_id_type=MESH)

    def load(src, dst, n):
        copy = pltpu.make_async_copy(src, dst, local_sem.at[n])
        copy.start()
        return copy

    load_gate = load(gate_hbm, gate_ref, 0)
    load_up = load(up_hbm, up_ref, 1)
    load_down = load(down_hbm, w_ref.at[2], 2)
    load_k = load(k_hbm, k_ref, 3)
    load_v = load(v_hbm, v_ref, 4)
    load_q = load(q_hbm, q_ref, 5)
    load_gain = load(gain_hbm, gain_ref, 6)
    with jax.named_scope("transpose"):
        load_gate.wait()
        load_up.wait()
        for first in range(0, gate_ref.shape[1], LANES):
            window = slice(first, first + LANES)
            w_ref[0, window, :] = gate_ref[:, window].T
            w_ref[1, window, :] = up_ref[:, window].T

    low_edge, high_edge = jnp.minimum(sp, 1), jnp.minimum(sp_count - 1 - sp, 1)
    with jax.named_scope("enter"):
        pl.semaphore_wait(barrier, 6 + low_edge + high_edge)
        load_down.wait()
        load_k.wait()
        load_v.wait()

    def remote(src, dst, ss, rs, dev):
        return pltpu.make_async_remote_copy(
            src_ref=src, dst_ref=dst, send_sem=ss, recv_sem=rs, device_id=dev, device_id_type=MESH
        )

    def arrived(copy, name):
        with jax.named_scope(name):
            copy.wait_recv()

    sent = []

    def start(copy):
        copy.start()
        sent.append(copy)

    win = khalo.shape[1]

    def halo(side, dev):
        first = rows - win if side == 0 else 0
        for n, (src, dst) in enumerate(((k_ref, khalo), (v_ref, vhalo))):
            m = 2 * side + n
            yield remote(
                src.at[first : first + win], dst.at[side], halo_ss.at[m], halo_rs.at[m], dev
            )

    @pl.when(sp < sp_count - 1)
    def _():
        for copy in halo(0, (sp + 1, c)):
            copy.start()

    @pl.when(sp > 0)
    def _():
        for copy in halo(1, (sp - 1, c)):
            copy.start()

    def role(dz, dx, dy):
        return (dz * 2 + dx) * 2 + dy

    def part(xx, qq, chunk):
        first = pl.multiple_of((xx * 2 + qq) * units + chunk[0], 64)
        return w_ref.at[:, pl.ds(first, chunk[1]), :]

    def slot(b, chunk):
        return wfull.at[b, :, chunk[0] : chunk[0] + chunk[1], :]

    def relay_slot(chunk):
        return wrelay.at[:, chunk[0] : chunk[0] + chunk[1], :]

    mine, from_x = place(z, y, x), place(z, y, xn)
    copies = {}
    for i, ch in enumerate(chunks):
        r = role(0, 1, 0)
        copies["x", i] = remote(part(xn, zq, ch), slot(mine, ch), w_ss.at[r, i], w_rs.at[r, i], to_x)
        copies["r", i] = remote(part(xn, 1 - zq, ch), relay_slot(ch), r_ss.at[i], r_rs.at[i], to_x)
        for dx, b in ((0, mine), (1, from_x)):
            for dz in (1, 2, 3):
                if dx == 0:
                    src = part(x, zq if dz == 2 else 1 - zq, ch)
                else:
                    src = slot(b, ch) if dz == 2 else relay_slot(ch)
                r = role(dz, dx, 0)
                copies["z", dx, dz, i] = remote(
                    src, slot(b, ch), w_ss.at[r, i], w_rs.at[r, i], to_z[dz]
                )

    z_of = [z, zn, zs, zf]
    OWN, NEAR, SAME, FAR = range(4)
    count = len(chunks)

    def wait_relay(i):
        window = relay_slot(chunks[i])
        remote(window, window, r_ss.at[i], r_rs.at[i], to_x).wait_recv()

    def block_of(dz, dx, dy):
        return place(z_of[dz], yn if dy else y, xn if dx else x)

    def wait_weights(dz, dx, dy, i):
        dst = slot(block_of(dz, dx, dy), chunks[i])
        r = role(dz, dx, dy)
        dev = to_y if dy else to_z[dz] if dz else to_x
        remote(dst, dst, w_ss.at[r, i], w_rs.at[r, i], dev).wait_recv()

    def to_y_copy(dz, dx, i):
        b = block_of(dz, dx, 0)
        src = part(x, zq, chunks[i]) if dz == dx == 0 else slot(b, chunks[i])
        r = role(dz, dx, 1)
        return remote(src, slot(b, chunks[i]), w_ss.at[r, i], w_rs.at[r, i], to_y)

    to_y_copies = {
        (dz, dx, i): to_y_copy(dz, dx, i)
        for dz in range(4) for dx in range(2) for i in range(count)
    }

    def y_relay(dz, dx, i):
        with jax.named_scope(f"y#dz={dz}#dx={dx}#i={i}"):
            wait_weights(dz, dx, 0, i)
            to_y_copies[dz, dx, i].start()

    def by_plane(step, outer, inner):
        @pl.when(zq == 0)
        def _():
            for key in outer:
                step(*key)

        @pl.when(zq == 1)
        def _():
            for key in inner:
                step(*key)

    def serve(outer, inner):
        by_plane(y_relay, outer, inner)

    def z_send(dz, dx, i):
        copies["z", dx, dz, i].start()

    def x_send(i):
        copies["x", i].start()
        copies["r", i].start()

    with jax.named_scope("issue"):
        for dz in (SAME, FAR, NEAR):
            z_send(dz, 0, 0)
        x_send(0)
        for i in range(count):
            to_y_copies[0, 0, i].start()

    load_ow = load(ow_hbm, ow, 7)
    own_weights = load(
        w_ref.at[:, pl.ds(pl.multiple_of((x * 2 + zq) * units, 64), units), :], wfull.at[mine], 8
    )
    load_res = load(res_hbm, dsend.at[0], 9)

    kv_here = k_ref.shape[1] // HEAD_DIM
    heads_here = q_ref.shape[1] // HEAD_DIM
    pairs = heads_here // kv_here // 2

    def spread(src, dst, first):
        count = src.shape[0]
        low = lax.broadcasted_iota(jnp.int32, (count, LANES), 1) < HEAD_DIM
        for j in range(kv_here // 2):
            t = src[:, j * LANES : (j + 1) * LANES].astype(f32)
            r = pltpu.roll(t, HEAD_DIM, 1)
            zero = jnp.zeros_like(t)
            window = slice(first, first + count)
            dst[2 * j, 0, window, :] = jnp.where(low, t, zero).astype(bf16)
            dst[2 * j, 1, window, :] = jnp.where(low, zero, r).astype(bf16)
            dst[2 * j + 1, 0, window, :] = jnp.where(low, r, zero).astype(bf16)
            dst[2 * j + 1, 1, window, :] = jnp.where(low, zero, t).astype(bf16)

    with jax.named_scope("spread"):
        spread(k_ref, exp_k, win)
        spread(v_ref, exp_v, win)

    def take_halo():
        @pl.when(sp > 0)
        def _():
            for copy in halo(0, (sp - 1, c)):
                arrived(copy, "halo")

        @pl.when(sp == 0)
        def _():
            khalo[0] = jnp.zeros_like(khalo[0])
            vhalo[0] = jnp.zeros_like(vhalo[0])

        @pl.when(sp < sp_count - 1)
        def _():
            for copy in halo(1, (sp + 1, c)):
                arrived(copy, "halo")

        @pl.when(sp == sp_count - 1)
        def _():
            khalo[1] = jnp.zeros_like(khalo[1])
            vhalo[1] = jnp.zeros_like(vhalo[1])

        for side, first in ((0, 0), (1, rows + win)):
            spread(khalo.at[side], exp_k, first)
            spread(vhalo.at[side], exp_v, first)

    total_rows = rows * sp_count

    def attend(blk):
        base = pl.multiple_of(blk * win, win)
        stack = (pairs * win, 3 * win)
        i = lax.broadcasted_iota(jnp.int32, stack, 0) % win
        j = lax.broadcasted_iota(jnp.int32, stack, 1)
        key = sp * rows + base - win + j
        valid = (j >= i) & (j <= i + 2 * win) & (key >= 0) & (key < total_rows)
        which = lax.broadcasted_iota(jnp.int32, (pairs * win, 1), 0) // win
        for g in range(kv_here):
            q2 = jnp.concatenate(
                [
                    q_ref[pl.ds(base, win), (g * pairs + p) * LANES : (g * pairs + p + 1) * LANES]
                    for p in range(pairs)
                ],
                axis=0,
            )
            out = None
            for side in range(2):
                kw = exp_k[g, side, pl.ds(base, 3 * win), :]
                scores = lax.dot_general(q2, kw, NT, preferred_element_type=f32) * HEAD_DIM**-0.5
                scores = jnp.where(valid, scores, -1e30)
                sink = jnp.zeros((pairs * win, 1), f32)
                for p in range(pairs):
                    sink = jnp.where(which == p, sink_ref[(g * pairs + p) * 2 + side], sink)
                peak = jnp.maximum(jnp.max(scores, axis=-1, keepdims=True), sink)
                weight = jnp.exp(scores - peak)
                denom = jnp.sum(weight, axis=-1, keepdims=True) + jnp.exp(sink - peak)
                probs = (weight * (1.0 / denom)).astype(bf16)
                vw = exp_v[g, side, pl.ds(base, 3 * win), :]
                got = jnp.dot(probs, vw, preferred_element_type=f32)
                out = got if out is None else out + got
            for p in range(pairs):
                att[pl.ds(base, win), (g * pairs + p) * LANES : (g * pairs + p + 1) * LANES] = out[
                    p * win : (p + 1) * win
                ].astype(bf16)

    def attend_step(n, carry):
        inner = rows // win - 2

        @pl.when(n == inner)
        def _():
            take_halo()

        attend(jnp.where(n < inner, n + 1, (n - inner) * (inner + 1)))

        @pl.when(n == 1)
        def _():
            x_send(1)
            by_plane(z_send, [], [(dz, 0, 1) for dz in (SAME, FAR, NEAR)])

        @pl.when(n == inner)
        def _():
            y_relay(OWN, 1, 0)
            wait_relay(0)
            for dz in (SAME, FAR, NEAR):
                z_send(dz, 1, 0)

        @pl.when(n == inner + 1)
        def _():
            for i in range(2, count):
                x_send(i)
            serve([(NEAR, 0, 0), (SAME, 0, 0)], [(SAME, 0, 0)])

        return carry

    with jax.named_scope("attention"):
        load_q.wait()
        lax.fori_loop(0, rows // win, attend_step, 0)

    depth = mixed.shape[1]
    tile = 4 * LANES
    load_ow.wait()
    load_gain.wait()
    other = pl.multiple_of((1 - c) * half, half)
    here = pl.multiple_of(c * half, half)
    for n in range(0, depth, tile):
        psend[:, n : n + tile] = jnp.dot(
            att[pl.ds(other, half), :], ow[:, n : n + tile], preferred_element_type=f32
        ).astype(bf16)
    swap_p = remote(psend, precv, p_ss.at[0], p_rs.at[0], partner)
    start(swap_p)
    load_res.wait()
    for n in range(0, depth, tile):
        partial_out = jnp.dot(
            att[pl.ds(here, half), :], ow[:, n : n + tile], preferred_element_type=f32
        )
        mixed[:, n : n + tile] = dsend[0, :, n : n + tile].astype(f32) + partial_out.astype(
            bf16
        ).astype(f32)
    arrived(swap_p, "swap")
    step = 64
    for m in range(0, half, step):
        part_mixed = mixed[m : m + step, :] + precv[m : m + step, :].astype(f32)
        mixed[m : m + step, :] = part_mixed
        inverse = lax.rsqrt(jnp.mean(part_mixed * part_mixed, axis=-1, keepdims=True) + 1e-06)
        tok[0, 0, m : m + step, :] = (part_mixed * inverse * gain_ref[...]).astype(bf16)

    def tok_copy(n, src, dst, dev):
        return remote(tok.at[src[0], src[1]], tok.at[dst[0], dst[1]], t_ss.at[n], t_rs.at[n], dev)

    t_x = tok_copy(0, (0, 0), (1, 0), to_x)
    t_z = tok_copy(1, (0, 0), (2, 0), to_z[1])
    t_d = tok_copy(2, (2, 0), (3, 0), to_x)
    t_p = [tok_copy(3 + g, (g, 0), (g, 1), partner) for g in range(4)]
    start(t_z)
    start(t_x)
    start(t_p[0])
    by_plane(z_send, [(dz, 0, 1) for dz in (SAME, FAR, NEAR)], [])
    for i in range(1, count):
        y_relay(OWN, 1, i)
        wait_relay(i)
        if i > 1:
            for dz in (SAME, FAR, NEAR):
                z_send(dz, 0, i)
        for dz in (SAME, FAR, NEAR):
            z_send(dz, 1, i)

    def weights_t(m, ch):
        lo, n = ch
        return jnp.concatenate([wfull[b, m, lo : lo + n, :] for b in range(blocks)], axis=1)

    def gate_up_rows(g, cc, i):
        lo, n = spans[i]
        t = tok[g, cc]
        gate = lax.dot_general(t, weights_t(0, spans[i]), NT, preferred_element_type=f32)
        upv = lax.dot_general(t, weights_t(1, spans[i]), NT, preferred_element_type=f32)
        hid[g, cc, :, lo : lo + n] = (gate / (1.0 + jnp.exp(-gate)) * upv).astype(bf16)

    def gate_up(g, i):
        def body(cc, carry):
            gate_up_rows(g, cc, i)
            return carry

        with jax.named_scope(f"gu#g={g}#i={i}"):
            lax.fori_loop(0, 2, body, 0)

    def project(g, cc, store):
        per = tile // width
        for n in range(0, blocks, per):
            wd = jnp.concatenate([wfull[b, 2] for b in range(n, n + per)], axis=1)
            store(
                slice(n * width, (n + per) * width),
                jnp.dot(hid[g, cc], wd, preferred_element_type=f32),
            )

    def ready(i):
        with jax.named_scope(f"ready#i={i}"):
            for dz in range(4):
                for dx in range(2):
                    wait_weights(dz, dx, 1, i)

    own_weights.wait()
    serve([(FAR, 0, 0)], [(FAR, 0, 0), (NEAR, 0, 0)])
    serve([(NEAR, 1, 0), (SAME, 1, 0), (NEAR, 0, 1)], [(SAME, 0, 1), (SAME, 1, 0), (FAR, 1, 0)])
    serve([(FAR, 0, 1), (FAR, 1, 0)], [(NEAR, 1, 0)])
    arrived(t_x, "t_x")
    start(t_p[1])
    ready(0)
    arrived(t_p[0], "t_p0")
    gate_up(0, 0)
    serve([(SAME, 0, 1)], [(SAME, 1, 1)])
    arrived(t_p[1], "t_p1")
    gate_up(1, 0)
    serve([(FAR, 1, 1), (SAME, 1, 1)], [(FAR, 0, 1)])
    arrived(t_z, "t_z")
    start(t_d)
    start(t_p[2])
    serve([(FAR, 0, 2)], [(NEAR, 0, 1), (SAME, 0, 2)])
    arrived(t_p[2], "t_p2")
    gate_up(2, 0)
    serve([(SAME, 0, 2), (NEAR, 1, 1)], [(FAR, 1, 1), (NEAR, 1, 1)])
    serve([(FAR, 1, 2), (SAME, 1, 2)], [(SAME, 1, 2)])
    serve([(NEAR, 0, 2), (FAR, 0, 3), (NEAR, 1, 2)], [(FAR, 0, 2), (NEAR, 0, 2)])
    ready(1)
    gate_up(0, 1)
    serve([(SAME, 0, 3)], [(FAR, 1, 2), (SAME, 0, 3)])
    gate_up(1, 1)
    serve([(NEAR, 0, 3), (SAME, 1, 3)], [(NEAR, 1, 2), (FAR, 0, 3)])
    gate_up(2, 1)
    serve([(FAR, 1, 3), (NEAR, 1, 3)], [(SAME, 1, 3), (NEAR, 0, 3), (FAR, 1, 3), (NEAR, 1, 3)])
    arrived(t_d, "t_d")
    start(t_p[3])
    ready(2)
    arrived(t_p[3], "t_p3")
    for i in range(len(spans) - 1):
        gate_up(3, i)
    for i in range(3, count):
        ready(i)

    quarter = half // 2
    last = len(spans) - 1
    parts = [slice(0, quarter), slice(quarter, half)]

    def to_partner(g, h):
        return remote(
            dsend.at[g, parts[h]], drecv.at[g, parts[h]], d_ss.at[g, h], d_rs.at[g, h], partner
        )

    def send_partner(g, order):
        def store(cols, value):
            dsend[g, :, cols] = value.astype(bf16)

        with jax.named_scope(f"send#g={g}"):
            gate_up_rows(g, 1, last)
            project(g, 1, store)
            for h in order:
                start(to_partner(g, h))

    def keep(g, n):
        def store(cols, value):
            own[n, :, cols] = value

        with jax.named_scope(f"keep#g={g}"):
            gate_up_rows(g, 0, last)
            project(g, 0, store)

    def summed(g, n, h):
        arrived(to_partner(g, h), f"partner#g={g}")
        return own[n, parts[h], :] + drecv[g, parts[h], :].astype(f32)

    e_x = remote(esend.at[0], erecv.at[0], e_ss.at[0], e_rs.at[0], to_x)
    e_z = remote(esend.at[1], erecv.at[1], e_ss.at[1], e_rs.at[1], to_z[1])

    def out_copy(n, h, dev):
        return remote(
            ssend.at[n, parts[h]], srecv.at[n, parts[h]], s_ss.at[n, h], s_rs.at[n, h], dev
        )

    out_x, out_z = out_copy(0, 0, to_x), [out_copy(1, h, to_z[1]) for h in range(2)]
    eighth = quarter // 2
    ends = [slice(quarter + n * eighth, quarter + (n + 1) * eighth) for n in range(2)]
    out_end = [
        remote(ssend.at[0, rows_], srecv.at[0, rows_], s_ss.at[0, 1 + n], s_rs.at[0, 1 + n], to_x)
        for n, rows_ in enumerate(ends)
    ]

    send_partner(3, (0, 1))
    keep(3, 2)
    for h, copy in enumerate((e_x, e_z)):
        esend[h] = summed(3, 2, h).astype(bf16)
        start(copy)
    send_partner(1, (0, 1))
    keep(1, 1)
    ssend[0, parts[0], :] = summed(1, 1, 0).astype(bf16)
    start(out_x)
    send_partner(2, (1, 0))
    keep(2, 0)
    ssend[1, parts[1], :] = summed(2, 0, 1).astype(bf16)
    start(out_z[1])
    send_partner(0, (0, 1))

    def add_mixed(cols, value):
        mixed[:, cols] = mixed[:, cols] + value

    gate_up_rows(0, 0, last)
    project(0, 0, add_mixed)
    own[1, parts[1], :] = summed(1, 1, 1)
    own[0, parts[0], :] = summed(2, 0, 0)
    for h in range(2):
        arrived(to_partner(0, h), "partner0")
    mixed[...] = mixed[...] + drecv[0].astype(f32)

    def pass_on(along_x):
        if along_x:
            arrived(e_z, "e_z")
            for n, copy in enumerate(out_end):
                got = erecv[1, n * eighth : (n + 1) * eighth, :].astype(f32)
                ssend[0, ends[n], :] = (own[1, ends[n], :] + got).astype(bf16)
                copy.start()
        else:
            arrived(e_x, "e_x")
            ssend[1, parts[0], :] = (own[0, parts[0], :] + erecv[0].astype(f32)).astype(bf16)
            out_z[0].start()

    by_plane(pass_on, [(True,), (False,)], [(False,), (True,)])
    sent.extend((*out_end, out_z[0]))
    arrived(out_x, "out_x")
    mixed[parts[0], :] = mixed[parts[0], :] + srecv[0, parts[0], :].astype(f32)
    arrived(out_z[1], "out_z1")
    mixed[parts[1], :] = mixed[parts[1], :] + srecv[1, parts[1], :].astype(f32)

    stores = []

    def finish(rows_, n):
        precv[rows_, :] = (mixed[rows_, :] + srecv[n, rows_, :].astype(f32)).astype(bf16)
        copy = pltpu.make_async_copy(
            precv.at[rows_], o_hbm.at[rows_], local_sem.at[len(stores)]
        )
        copy.start()
        stores.append(copy)

    arrived(out_z[0], "out_z0")
    finish(parts[0], 1)
    for n, copy in enumerate(out_end):
        arrived(copy, "out_end")
        finish(ends[n], 0)

    for copy in [*sent, *copies.values(), *to_y_copies.values()]:
        copy.wait_send()

    @pl.when(sp < sp_count - 1)
    def _():
        for copy in halo(0, (sp + 1, c)):
            copy.wait_send()

    @pl.when(sp > 0)
    def _():
        for copy in halo(1, (sp - 1, c)):
            copy.wait_send()

    for copy in stores:
        copy.wait()


def fused_shards(
    queries, key_rows, values, sink_logit, residual_in, out_weight, norm_gain,
    gate_weight, up_weight, down_weight,
):
    bf16, f32 = jnp.bfloat16, jnp.float32
    rows, depth = queries.shape[0], residual_in.shape[1]
    half = residual_in.shape[0]
    blocks = lax.axis_size("sp")
    kv = key_rows.shape[1]
    kv_here = kv // HEAD_DIM
    width = down_weight.shape[1]
    units = down_weight.shape[0] // 4
    count = len(chunks_of(units))
    smem = pl.BlockSpec(memory_space=pltpu.SMEM)
    hbm = pl.BlockSpec(memory_space=pl.ANY)
    dma = pltpu.SemaphoreType.DMA
    scratch = [
        pltpu.VMEM(key_rows.shape, bf16),
        pltpu.VMEM(values.shape, bf16),
        pltpu.VMEM((1, depth), f32),
        pltpu.VMEM(gate_weight.shape, bf16),
        pltpu.VMEM(up_weight.shape, bf16),
        pltpu.VMEM((3, down_weight.shape[0], width), bf16),
        pltpu.VMEM(queries.shape, bf16),
        pltpu.VMEM((2, WINDOW, kv), bf16),
        pltpu.VMEM((2, WINDOW, kv), bf16),
        pltpu.VMEM((kv_here, 2, rows + 2 * WINDOW, LANES), bf16),
        pltpu.VMEM((kv_here, 2, rows + 2 * WINDOW, LANES), bf16),
        pltpu.VMEM(queries.shape, bf16),
        pltpu.VMEM(out_weight.shape, bf16),
        pltpu.VMEM((half, depth), bf16),
        pltpu.VMEM((half, depth), bf16),
        pltpu.VMEM((half, depth), f32),
        pltpu.VMEM((4, 2, half, depth), bf16),
        pltpu.VMEM((blocks, 3, units, width), bf16),
        pltpu.VMEM((3, units, width), bf16),
        pltpu.VMEM((4, 2, half, units), bf16),
        pltpu.VMEM((4, half, depth), bf16),
        pltpu.VMEM((4, half, depth), bf16),
        pltpu.VMEM((3, half, depth), f32),
        pltpu.VMEM((2, half // 2, depth), bf16),
        pltpu.VMEM((2, half // 2, depth), bf16),
        pltpu.VMEM((2, half, depth), bf16),
        pltpu.VMEM((2, half, depth), bf16),
        dma((12,)), dma((4,)), dma((4,)), dma((1,)), dma((1,)),
        dma((16, count)), dma((16, count)), dma((count,)), dma((count,)),
        dma((7,)), dma((7,)), dma((4, 2)), dma((4, 2)), dma((2,)), dma((2,)),
        dma((2, 3)), dma((2, 3)),
    ]
    return pl.pallas_call(
        fused,
        out_shape=jax.ShapeDtypeStruct(residual_in.shape, bf16),
        in_specs=[hbm, hbm, hbm, smem, hbm, hbm, hbm, hbm, hbm, hbm],
        out_specs=hbm,
        scratch_shapes=scratch,
        compiler_params=pltpu.CompilerParams(
            collective_id=0, has_side_effects=True, vmem_limit_bytes=63 * 1024 * 1024
        ),
    )(
        queries, key_rows, values, sink_logit, residual_in, out_weight,
        norm_gain.reshape(1, depth), gate_weight, up_weight, down_weight,
    )


def solution(mesh):
    sp_count, tp_count = mesh.shape["sp"], mesh.shape["tp"]
    group = math.gcd(sp_count, 4)
    if tp_count == 2 and sp_count == 4 * group:
        return jax.shard_map(
            fused_shards,
            mesh=mesh,
            in_specs=(
                P("sp", "tp"),
                P("sp", "tp"),
                P("sp", "tp"),
                P("tp"),
                P(("sp", "tp"), None),
                P("tp", None),
                P(),
                P("sp", "tp"),
                P("sp", "tp"),
                P("tp", "sp"),
            ),
            out_specs=P(("sp", "tp"), None),
            check_vma=False,
        )
    fine = Mesh(mesh.devices.reshape(sp_count // group, group, tp_count), ("o", "q", "tp"))
    sp = ("o", "q")
    return jax.shard_map(
        shards,
        mesh=fine,
        in_specs=(
            P(sp, "tp"),
            P(sp, "tp"),
            P(sp, "tp"),
            P("tp"),
            P(("o", "q", "tp"), None),
            P("tp", None),
            P(),
            P(sp, "tp"),
            P(sp, "tp"),
            P("tp", sp),
        ),
        out_specs=P(("o", "q", "tp"), None),
        check_vma=False,
    )
```

```python
import math

import jax
import jax.numpy as jnp
from jax import lax
from jax.experimental import pallas as pl
from jax.experimental.pallas import tpu as pltpu
from jax.sharding import Mesh
from jax.sharding import PartitionSpec as P

HEAD_DIM = 64
WINDOW = 128


def with_halo(block, sides, width):
    for axis, dim in sides:
        count = math.prod(lax.axis_size(name) for name in axis)
        forward = [(i, i + 1) for i in range(count - 1)]
        backward = [(target, source) for source, target in forward]
        low = lax.ppermute(
            lax.slice_in_dim(block, block.shape[dim] - width, None, axis=dim), axis, forward
        )
        high = lax.ppermute(lax.slice_in_dim(block, 0, width, axis=dim), axis, backward)
        block = jnp.concatenate([low, block, high], axis=dim)
    return block


def rms_scale(mixed_rows, norm_gain):
    inverse = lax.rsqrt(jnp.mean(mixed_rows * mixed_rows, axis=-1, keepdims=True) + 1e-06)
    return (mixed_rows * inverse * norm_gain).astype(jnp.bfloat16)


def attend_window(queries, padded, offset, total_rows, sink_logit, between):
    rows_here = queries.shape[0]
    block_count = rows_here // WINDOW
    heads_here = queries.shape[1] // HEAD_DIM
    kv_here = padded.shape[1] // (2 * HEAD_DIM)
    group_size = heads_here // kv_here
    blocks = padded.reshape(block_count + 2, WINDOW, padded.shape[1])
    banded = jnp.concatenate([blocks[:-2], blocks[1:-1], blocks[2:]], axis=1)
    key_band = banded[:, :, : kv_here * HEAD_DIM].reshape(
        block_count, 3 * WINDOW, kv_here, HEAD_DIM
    )
    value_band = banded[:, :, kv_here * HEAD_DIM :].reshape(
        block_count, 3 * WINDOW, kv_here, HEAD_DIM
    )
    grouped = queries.reshape(block_count, WINDOW, kv_here, group_size, HEAD_DIM)
    scores = jnp.einsum(
        "nqkgd,nskd->nkgqs", grouped, key_band, preferred_element_type=jnp.float32
    ) * HEAD_DIM ** (-0.5)
    scores, moved = lax.optimization_barrier((scores, between))
    block_start = offset + jnp.arange(block_count, dtype=jnp.int32)[:, None] * WINDOW
    query_pos = block_start + jnp.arange(WINDOW, dtype=jnp.int32)[None, :]
    key_pos = block_start - WINDOW + jnp.arange(3 * WINDOW, dtype=jnp.int32)[None, :]
    valid = jnp.abs(query_pos[:, :, None] - key_pos[:, None, :]) <= WINDOW
    valid = valid & ((key_pos >= 0) & (key_pos < total_rows))[:, None, :]
    scores = jnp.where(valid[:, None, None], scores, -1e30)
    sink_grid = sink_logit.reshape(kv_here, group_size)[None, :, :, None, None]
    peak = jnp.maximum(jnp.max(scores, axis=-1, keepdims=True), sink_grid)
    weights_raw = jnp.exp(scores - peak)
    denom = jnp.sum(weights_raw, axis=-1, keepdims=True) + jnp.exp(sink_grid - peak)
    probs = (weights_raw / denom).astype(jnp.bfloat16)
    output = jnp.einsum("nkgqs,nskd->nqkgd", probs, value_band, preferred_element_type=jnp.float32)
    return output.astype(jnp.bfloat16).reshape(rows_here, heads_here * HEAD_DIM), moved


def swap(array, axis, distance):
    count = lax.axis_size(axis)
    return lax.ppermute(array, axis, [(i, i ^ distance) for i in range(count)])


def turn(array, step):
    count = lax.axis_size("o")
    return lax.ppermute(array, "o", [(i, (i + step) % count) for i in range(count)])


def piece(array, index, size, dim):
    return lax.dynamic_slice_in_dim(array, index * size, size, dim)


def shards(
    queries,
    key_rows,
    values,
    sink_logit,
    residual_in,
    out_weight,
    norm_gain,
    gate_weight,
    up_weight,
    down_weight,
):
    rows_here = queries.shape[0]
    tp_count, group = lax.axis_size("tp"), lax.axis_size("q")
    row_share = rows_here // tp_count
    q_index, tp_index = lax.axis_index("q"), lax.axis_index("tp")
    units = gate_weight.shape[1] // group

    joined = jnp.concatenate([key_rows, values], axis=1)
    padded = with_halo(joined, ((("o", "q"), 0),), WINDOW)

    gate_up = jnp.stack([gate_weight, up_weight])
    gate_up_got, down_got = [], []
    for k in range(group):
        part = piece(gate_up, q_index ^ k, units, 2)
        gate_up_got.append(swap(part, "q", k) if k else part)
    for k in range(group):
        part = piece(down_weight, q_index ^ k, units, 0)
        down_got.append(swap(part, "q", k) if k else part)
    depth, width = gate_weight.shape[0], down_weight.shape[1]
    gate_up_mine = jnp.zeros((2, group * depth, units), gate_weight.dtype)
    down_mine = jnp.zeros((units, group * width), down_weight.dtype)
    for k in range(group):
        gate_up_mine = lax.dynamic_update_slice_in_dim(
            gate_up_mine, gate_up_got[k], (q_index ^ k) * depth, 1
        )
        down_mine = lax.dynamic_update_slice_in_dim(
            down_mine, down_got[k], (q_index ^ k) * width, 1
        )
    sp_index = lax.axis_index(("o", "q"))
    total_rows = rows_here * lax.axis_size(("o", "q"))
    mine = (gate_up_mine[0], gate_up_mine[1], down_mine)
    attended, mine = attend_window(
        queries, padded, sp_index * rows_here, total_rows, sink_logit, mine
    )
    outer = lax.axis_size("o")
    pieces = [(0, mine)]
    rings = [(x, x) for x in mine]
    if outer > 2:
        rings = [(turn(x, 1), turn(x, -1)) for x in mine]
        attended, rings[0] = lax.optimization_barrier((attended, rings[0]))

    partial_value = jnp.dot(attended, out_weight, preferred_element_type=jnp.float32).astype(
        jnp.bfloat16
    )
    mixed = residual_in.astype(jnp.float32) + piece(partial_value, tp_index, row_share, 0).astype(
        jnp.float32
    )
    for j in range(1, tp_count):
        sent = piece(partial_value, tp_index ^ j, row_share, 0)
        mixed = mixed + swap(sent, "tp", j).astype(jnp.float32)
    normed = rms_scale(mixed, norm_gain)

    own = normed
    if outer > 2:
        own, rings[1] = lax.optimization_barrier((normed, rings[1]))
        pieces += [(-1, [x for x, _ in rings]), (1, [y for _, y in rings])]
    for distance in range(2, (outer - 1) // 2 + 1):
        rings = [(turn(x, 1), turn(y, -1)) for x, y in rings]
        pieces += [(-distance, [x for x, _ in rings]), (distance, [y for _, y in rings])]
    if outer > 1 and outer % 2 == 0:
        far = []
        for x, y in rings:
            half = x.shape[0] // 2
            far.append(jnp.concatenate([turn(x[:half], 1), turn(y[half:], -1)], axis=0))
        pieces.append((outer // 2, far))
    gate_full = jnp.zeros((outer * group * depth, units), gate_weight.dtype)
    up_full = jnp.zeros((outer * group * depth, units), gate_weight.dtype)
    down_full = jnp.zeros((units, outer * group * width), down_weight.dtype)
    for distance, (gate_part, up_part, down_part) in pieces:
        place = lax.rem(lax.axis_index("o") + distance + outer, outer)
        row = place * group * depth
        gate_full = lax.dynamic_update_slice_in_dim(gate_full, gate_part, row, 0)
        up_full = lax.dynamic_update_slice_in_dim(up_full, up_part, row, 0)
        down_full = lax.dynamic_update_slice_in_dim(down_full, down_part, place * group * width, 1)

    order = [*range(group - 1, 0, -1), 0]
    arrived = {k: swap(normed, "q", k) for k in order if k}
    arrived[0] = own
    result = mixed
    waiting, received = None, []
    for k in order:
        rows = jnp.concatenate(
            [swap(arrived[k], "tp", j) if j else arrived[k] for j in range(tp_count)], axis=0
        )
        gate_pre = jnp.dot(rows, gate_full, preferred_element_type=jnp.float32)
        up_pre = jnp.dot(rows, up_full, preferred_element_type=jnp.float32)
        hidden = (jax.nn.silu(gate_pre) * up_pre).astype(jnp.bfloat16)
        if waiting is not None:
            sent, hidden = lax.optimization_barrier((waiting[1], hidden))
            received.append(swap(sent, "q", waiting[0]))
        if k == 0 and len(received) > 2:
            received[0], hidden = lax.optimization_barrier((received[0], hidden))
        parts = []
        for j in [*range(1, tp_count), 0]:
            if j == k == 0 and len(received) > 2:
                received[1], parts, hidden = lax.optimization_barrier(
                    (received[1], parts, hidden)
                )
            share = hidden[j * row_share : (j + 1) * row_share]
            out = jnp.dot(share, down_full, preferred_element_type=jnp.float32)
            out = out.astype(jnp.bfloat16)
            parts.append(swap(out, "tp", j) if j else out)
        total = sum(part.astype(jnp.float32) for part in parts)
        if k:
            waiting = (k, total.astype(jnp.bfloat16))
        else:
            result = result + total
    for part in received:
        result = result + part.astype(jnp.float32)
    return result.astype(jnp.bfloat16)


MESH = pl.DeviceIdType.MESH
LANES = 128
NT = (((1,), (1,)), ((), ()))


def spans_of(units):
    step = 2 * LANES
    return [(start, min(step, units - start)) for start in range(0, units, step)]


def chunks_of(units):
    *full, (start, size) = spans_of(units)
    first = min(size, LANES)
    return [*full, (start, first)] + [(start + first, size - first)] * (size > first)


def fused(
    q_hbm, k_hbm, v_hbm, sink_ref, res_hbm, ow_hbm, gain_hbm, gate_hbm, up_hbm, down_hbm, o_ref,
    k_ref, v_ref, gain_ref, gate_ref, up_ref, w_ref, q_ref, khalo, vhalo, exp_k, exp_v, att, ow, psend, precv, mixed,
    tok, wfull, wrelay, hid, dsend, drecv, own, esend, erecv, ssend, srecv,
    local_sem, halo_ss, halo_rs, p_ss, p_rs, w_ss, w_rs, r_ss, r_rs,
    t_ss, t_rs, d_ss, d_rs, e_ss, e_rs, s_ss, s_rs,
):
    f32, bf16 = jnp.float32, jnp.bfloat16
    sp, c = lax.axis_index("sp"), lax.axis_index("tp")
    sp_count = lax.axis_size("sp")
    x, y, z = sp % 2, (sp // 2) % 2, sp // 4
    xn, yn, zn, zs = 1 - x, 1 - y, z + 1 - 2 * (z % 2), 3 - z
    zf = 3 - zn
    zq = (z * (3 - z)) // 2
    rows = q_ref.shape[0]
    half = rows // 2
    units = wfull.shape[2]
    chunks, spans = chunks_of(units), spans_of(units)
    width = wfull.shape[3]
    blocks = wfull.shape[0]

    def place(zz, yy, xx):
        return (zz * 2 + yy) * 2 + xx

    partner = (sp, 1 - c)
    to_x, to_y = (place(z, y, xn), c), (place(z, yn, x), c)
    to_z = [None, (place(zn, y, x), c), (place(zs, y, x), c), (place(zf, y, x), c)]

    barrier = pltpu.get_barrier_semaphore()
    for peer in (partner, to_x, to_y, to_z[1], to_z[2], to_z[3]):
        pl.semaphore_signal(barrier, inc=1, device_id=peer, device_id_type=MESH)

    @pl.when(sp > 0)
    def _():
        pl.semaphore_signal(barrier, inc=1, device_id=(sp - 1, c), device_id_type=MESH)

    @pl.when(sp < sp_count - 1)
    def _():
        pl.semaphore_signal(barrier, inc=1, device_id=(sp + 1, c), device_id_type=MESH)

    def load(src, dst, n):
        copy = pltpu.make_async_copy(src, dst, local_sem.at[n])
        copy.start()
        return copy

    load_gate = load(gate_hbm, gate_ref, 0)
    load_up = load(up_hbm, up_ref, 1)
    load_down = load(down_hbm, w_ref.at[2], 2)
    load_k = load(k_hbm, k_ref, 3)
    load_v = load(v_hbm, v_ref, 4)
    load_q = load(q_hbm, q_ref, 5)
    load_gain = load(gain_hbm, gain_ref, 6)
    with jax.named_scope("transpose"):
        load_gate.wait()
        load_up.wait()
        for first in range(0, gate_ref.shape[1], LANES):
            window = slice(first, first + LANES)
            w_ref[0, window, :] = gate_ref[:, window].T
            w_ref[1, window, :] = up_ref[:, window].T

    low_edge, high_edge = jnp.minimum(sp, 1), jnp.minimum(sp_count - 1 - sp, 1)
    with jax.named_scope("enter"):
        pl.semaphore_wait(barrier, 6 + low_edge + high_edge)
        load_down.wait()
        load_k.wait()
        load_v.wait()

    def remote(src, dst, ss, rs, dev):
        return pltpu.make_async_remote_copy(
            src_ref=src, dst_ref=dst, send_sem=ss, recv_sem=rs, device_id=dev, device_id_type=MESH
        )

    def arrived(copy, name):
        with jax.named_scope(name):
            copy.wait_recv()

    sent = []

    def start(copy):
        copy.start()
        sent.append(copy)

    win = khalo.shape[1]

    def halo(side, dev):
        first = rows - win if side == 0 else 0
        for n, (src, dst) in enumerate(((k_ref, khalo), (v_ref, vhalo))):
            m = 2 * side + n
            yield remote(
                src.at[first : first + win], dst.at[side], halo_ss.at[m], halo_rs.at[m], dev
            )

    @pl.when(sp < sp_count - 1)
    def _():
        for copy in halo(0, (sp + 1, c)):
            copy.start()

    @pl.when(sp > 0)
    def _():
        for copy in halo(1, (sp - 1, c)):
            copy.start()

    def role(dz, dx, dy):
        return (dz * 2 + dx) * 2 + dy

    def part(xx, qq, chunk):
        first = pl.multiple_of((xx * 2 + qq) * units + chunk[0], 64)
        return w_ref.at[:, pl.ds(first, chunk[1]), :]

    def slot(b, chunk):
        return wfull.at[b, :, chunk[0] : chunk[0] + chunk[1], :]

    def relay_slot(chunk):
        return wrelay.at[:, chunk[0] : chunk[0] + chunk[1], :]

    mine, from_x = place(z, y, x), place(z, y, xn)
    copies = {}
    for i, ch in enumerate(chunks):
        r = role(0, 1, 0)
        copies["x", i] = remote(part(xn, zq, ch), slot(mine, ch), w_ss.at[r, i], w_rs.at[r, i], to_x)
        copies["r", i] = remote(part(xn, 1 - zq, ch), relay_slot(ch), r_ss.at[i], r_rs.at[i], to_x)
        for dx, b in ((0, mine), (1, from_x)):
            for dz in (1, 2, 3):
                if dx == 0:
                    src = part(x, zq if dz == 2 else 1 - zq, ch)
                else:
                    src = slot(b, ch) if dz == 2 else relay_slot(ch)
                r = role(dz, dx, 0)
                copies["z", dx, dz, i] = remote(
                    src, slot(b, ch), w_ss.at[r, i], w_rs.at[r, i], to_z[dz]
                )

    z_of = [z, zn, zs, zf]
    OWN, NEAR, SAME, FAR = range(4)
    count = len(chunks)

    def wait_relay(i):
        window = relay_slot(chunks[i])
        remote(window, window, r_ss.at[i], r_rs.at[i], to_x).wait_recv()

    def block_of(dz, dx, dy):
        return place(z_of[dz], yn if dy else y, xn if dx else x)

    def wait_weights(dz, dx, dy, i):
        dst = slot(block_of(dz, dx, dy), chunks[i])
        r = role(dz, dx, dy)
        dev = to_y if dy else to_z[dz] if dz else to_x
        remote(dst, dst, w_ss.at[r, i], w_rs.at[r, i], dev).wait_recv()

    def to_y_copy(dz, dx, i):
        b = block_of(dz, dx, 0)
        src = part(x, zq, chunks[i]) if dz == dx == 0 else slot(b, chunks[i])
        r = role(dz, dx, 1)
        return remote(src, slot(b, chunks[i]), w_ss.at[r, i], w_rs.at[r, i], to_y)

    to_y_copies = {
        (dz, dx, i): to_y_copy(dz, dx, i)
        for dz in range(4) for dx in range(2) for i in range(count)
    }

    def y_relay(dz, dx, i):
        with jax.named_scope(f"y#dz={dz}#dx={dx}#i={i}"):
            wait_weights(dz, dx, 0, i)
            to_y_copies[dz, dx, i].start()

    def by_plane(step, outer, inner):
        @pl.when(zq == 0)
        def _():
            for key in outer:
                step(*key)

        @pl.when(zq == 1)
        def _():
            for key in inner:
                step(*key)

    def serve(outer, inner):
        by_plane(y_relay, outer, inner)

    def z_send(dz, dx, i):
        copies["z", dx, dz, i].start()

    def x_send(i):
        copies["x", i].start()
        copies["r", i].start()

    with jax.named_scope("issue"):
        for dz in (SAME, FAR, NEAR):
            z_send(dz, 0, 0)
        x_send(0)
        for i in range(count):
            to_y_copies[0, 0, i].start()

    load_ow = load(ow_hbm, ow, 7)
    own_weights = load(
        w_ref.at[:, pl.ds(pl.multiple_of((x * 2 + zq) * units, 64), units), :], wfull.at[mine], 8
    )
    load_res = load(res_hbm, dsend.at[0], 9)

    kv_here = k_ref.shape[1] // HEAD_DIM
    heads_here = q_ref.shape[1] // HEAD_DIM
    pairs = heads_here // kv_here // 2

    def spread(src, dst, first):
        count = src.shape[0]
        low = lax.broadcasted_iota(jnp.int32, (count, LANES), 1) < HEAD_DIM
        for j in range(kv_here // 2):
            t = src[:, j * LANES : (j + 1) * LANES].astype(f32)
            r = pltpu.roll(t, HEAD_DIM, 1)
            zero = jnp.zeros_like(t)
            window = slice(first, first + count)
            dst[2 * j, 0, window, :] = jnp.where(low, t, zero).astype(bf16)
            dst[2 * j, 1, window, :] = jnp.where(low, zero, r).astype(bf16)
            dst[2 * j + 1, 0, window, :] = jnp.where(low, r, zero).astype(bf16)
            dst[2 * j + 1, 1, window, :] = jnp.where(low, zero, t).astype(bf16)

    with jax.named_scope("spread"):
        spread(k_ref, exp_k, win)
        spread(v_ref, exp_v, win)

    def take_halo():
        @pl.when(sp > 0)
        def _():
            for copy in halo(0, (sp - 1, c)):
                arrived(copy, "halo")

        @pl.when(sp == 0)
        def _():
            khalo[0] = jnp.zeros_like(khalo[0])
            vhalo[0] = jnp.zeros_like(vhalo[0])

        @pl.when(sp < sp_count - 1)
        def _():
            for copy in halo(1, (sp + 1, c)):
                arrived(copy, "halo")

        @pl.when(sp == sp_count - 1)
        def _():
            khalo[1] = jnp.zeros_like(khalo[1])
            vhalo[1] = jnp.zeros_like(vhalo[1])

        for side, first in ((0, 0), (1, rows + win)):
            spread(khalo.at[side], exp_k, first)
            spread(vhalo.at[side], exp_v, first)

    total_rows = rows * sp_count

    def attend(blk):
        base = pl.multiple_of(blk * win, win)
        stack = (pairs * win, 3 * win)
        i = lax.broadcasted_iota(jnp.int32, stack, 0) % win
        j = lax.broadcasted_iota(jnp.int32, stack, 1)
        key = sp * rows + base - win + j
        valid = (j >= i) & (j <= i + 2 * win) & (key >= 0) & (key < total_rows)
        which = lax.broadcasted_iota(jnp.int32, (pairs * win, 1), 0) // win
        for g in range(kv_here):
            q2 = jnp.concatenate(
                [
                    q_ref[pl.ds(base, win), (g * pairs + p) * LANES : (g * pairs + p + 1) * LANES]
                    for p in range(pairs)
                ],
                axis=0,
            )
            out = None
            for side in range(2):
                kw = exp_k[g, side, pl.ds(base, 3 * win), :]
                scores = lax.dot_general(q2, kw, NT, preferred_element_type=f32) * HEAD_DIM**-0.5
                scores = jnp.where(valid, scores, -1e30)
                sink = jnp.zeros((pairs * win, 1), f32)
                for p in range(pairs):
                    sink = jnp.where(which == p, sink_ref[(g * pairs + p) * 2 + side], sink)
                peak = jnp.maximum(jnp.max(scores, axis=-1, keepdims=True), sink)
                weight = jnp.exp(scores - peak)
                denom = jnp.sum(weight, axis=-1, keepdims=True) + jnp.exp(sink - peak)
                probs = (weight * (1.0 / denom)).astype(bf16)
                vw = exp_v[g, side, pl.ds(base, 3 * win), :]
                got = jnp.dot(probs, vw, preferred_element_type=f32)
                out = got if out is None else out + got
            for p in range(pairs):
                att[pl.ds(base, win), (g * pairs + p) * LANES : (g * pairs + p + 1) * LANES] = out[
                    p * win : (p + 1) * win
                ].astype(bf16)

    def attend_step(n, carry):
        inner = rows // win - 2

        @pl.when(n == inner)
        def _():
            take_halo()

        attend(jnp.where(n < inner, n + 1, (n - inner) * (inner + 1)))

        @pl.when(n == 1)
        def _():
            x_send(1)
            by_plane(z_send, [], [(dz, 0, 1) for dz in (SAME, FAR, NEAR)])

        @pl.when(n == inner)
        def _():
            y_relay(OWN, 1, 0)
            wait_relay(0)
            for dz in (SAME, FAR, NEAR):
                z_send(dz, 1, 0)

        @pl.when(n == inner + 1)
        def _():
            for i in range(2, count):
                x_send(i)
            serve([(NEAR, 0, 0), (SAME, 0, 0)], [(SAME, 0, 0)])

        return carry

    with jax.named_scope("attention"):
        load_q.wait()
        lax.fori_loop(0, rows // win, attend_step, 0)

    depth = mixed.shape[1]
    tile = 4 * LANES
    load_ow.wait()
    load_gain.wait()
    other = pl.multiple_of((1 - c) * half, half)
    here = pl.multiple_of(c * half, half)
    for n in range(0, depth, tile):
        psend[:, n : n + tile] = jnp.dot(
            att[pl.ds(other, half), :], ow[:, n : n + tile], preferred_element_type=f32
        ).astype(bf16)
    swap_p = remote(psend, precv, p_ss.at[0], p_rs.at[0], partner)
    start(swap_p)
    load_res.wait()
    for n in range(0, depth, tile):
        partial_out = jnp.dot(
            att[pl.ds(here, half), :], ow[:, n : n + tile], preferred_element_type=f32
        )
        mixed[:, n : n + tile] = dsend[0, :, n : n + tile].astype(f32) + partial_out.astype(
            bf16
        ).astype(f32)
    arrived(swap_p, "swap")
    step = 64
    for m in range(0, half, step):
        part_mixed = mixed[m : m + step, :] + precv[m : m + step, :].astype(f32)
        mixed[m : m + step, :] = part_mixed
        inverse = lax.rsqrt(jnp.mean(part_mixed * part_mixed, axis=-1, keepdims=True) + 1e-06)
        tok[0, 0, m : m + step, :] = (part_mixed * inverse * gain_ref[...]).astype(bf16)

    def tok_copy(n, src, dst, dev):
        return remote(tok.at[src[0], src[1]], tok.at[dst[0], dst[1]], t_ss.at[n], t_rs.at[n], dev)

    t_x = tok_copy(0, (0, 0), (1, 0), to_x)
    pieces = [slice(0, half // 2), slice(half // 2, half)]

    def tok_piece(n, src, dst, dev):
        return [
            remote(
                tok.at[src, 0, rows_], tok.at[dst, 0, rows_], t_ss.at[n + h], t_rs.at[n + h], dev
            )
            for h, rows_ in enumerate(pieces)
        ]

    t_z = tok_piece(1, 0, 2, to_z[1])
    t_d = tok_piece(7, 2, 3, to_x)
    t_p = [tok_copy(3 + g, (g, 0), (g, 1), partner) for g in range(4)]
    start(t_z[0])
    start(t_z[1])
    start(t_x)
    start(t_p[0])
    by_plane(z_send, [(dz, 0, 1) for dz in (SAME, FAR, NEAR)], [])
    for i in range(1, count):
        y_relay(OWN, 1, i)
        wait_relay(i)
        if i > 1:
            for dz in (SAME, FAR, NEAR):
                z_send(dz, 0, i)
        for dz in (SAME, FAR, NEAR):
            z_send(dz, 1, i)

    def weights_t(m, ch):
        lo, n = ch
        return jnp.concatenate([wfull[b, m, lo : lo + n, :] for b in range(blocks)], axis=1)

    def gate_up_rows(g, cc, i):
        lo, n = spans[i]
        t = tok[g, cc]
        gate = lax.dot_general(t, weights_t(0, spans[i]), NT, preferred_element_type=f32)
        upv = lax.dot_general(t, weights_t(1, spans[i]), NT, preferred_element_type=f32)
        hid[g, cc, :, lo : lo + n] = (gate / (1.0 + jnp.exp(-gate)) * upv).astype(bf16)

    def gate_up(g, i):
        def body(cc, carry):
            gate_up_rows(g, cc, i)
            return carry

        with jax.named_scope(f"gu#g={g}#i={i}"):
            lax.fori_loop(0, 2, body, 0)

    def project(g, cc, store):
        per = tile // width
        for n in range(0, blocks, per):
            wd = jnp.concatenate([wfull[b, 2] for b in range(n, n + per)], axis=1)
            store(
                slice(n * width, (n + per) * width),
                jnp.dot(hid[g, cc], wd, preferred_element_type=f32),
            )

    def ready(i):
        with jax.named_scope(f"ready#i={i}"):
            for dz in range(4):
                for dx in range(2):
                    wait_weights(dz, dx, 1, i)

    own_weights.wait()
    serve([(FAR, 0, 0)], [(FAR, 0, 0), (NEAR, 0, 0)])
    serve([(NEAR, 1, 0), (SAME, 1, 0), (NEAR, 0, 1)], [(SAME, 0, 1), (SAME, 1, 0), (FAR, 1, 0)])
    serve([(FAR, 0, 1), (FAR, 1, 0)], [(NEAR, 1, 0)])
    arrived(t_x, "t_x")
    start(t_p[1])
    ready(0)
    arrived(t_p[0], "t_p0")
    gate_up(0, 0)
    arrived(t_z[0], "t_z0")
    start(t_d[0])
    serve([(SAME, 0, 1)], [(SAME, 1, 1)])
    arrived(t_p[1], "t_p1")
    gate_up(1, 0)
    serve([(FAR, 1, 1), (SAME, 1, 1)], [(FAR, 0, 1)])
    arrived(t_z[1], "t_z1")
    start(t_d[1])
    start(t_p[2])
    serve([(FAR, 0, 2)], [(NEAR, 0, 1), (SAME, 0, 2)])
    arrived(t_p[2], "t_p2")
    gate_up(2, 0)
    serve([(SAME, 0, 2), (NEAR, 1, 1)], [(FAR, 1, 1), (NEAR, 1, 1)])
    serve([(FAR, 1, 2), (SAME, 1, 2)], [(SAME, 1, 2)])
    serve([(NEAR, 0, 2)], [(FAR, 0, 2), (NEAR, 0, 2)])
    ready(1)
    gate_up(0, 1)
    serve([(NEAR, 1, 2)], [(FAR, 1, 2), (SAME, 0, 3)])
    gate_up(1, 1)
    for copy in t_d:
        arrived(copy, "t_d")
    start(t_p[3])
    serve([(FAR, 0, 3), (SAME, 0, 3)], [(NEAR, 1, 2), (FAR, 0, 3)])
    gate_up(2, 1)
    serve(
        [(NEAR, 0, 3), (SAME, 1, 3), (FAR, 1, 3), (NEAR, 1, 3)],
        [(SAME, 1, 3), (NEAR, 0, 3), (FAR, 1, 3), (NEAR, 1, 3)],
    )
    arrived(t_p[3], "t_p3")
    for i in range(len(spans) - 1):
        gate_up(3, i)
    for i in range(2, count):
        ready(i)

    quarter = half // 2
    last = len(spans) - 1
    parts = [slice(0, quarter), slice(quarter, half)]

    def to_partner(g, h):
        return remote(
            dsend.at[g, parts[h]], drecv.at[g, parts[h]], d_ss.at[g, h], d_rs.at[g, h], partner
        )

    def send_partner(g, order):
        def store(cols, value):
            dsend[g, :, cols] = value.astype(bf16)

        with jax.named_scope(f"send#g={g}"):
            gate_up_rows(g, 1, last)
            project(g, 1, store)
            for h in order:
                start(to_partner(g, h))

    def keep(g, n):
        def store(cols, value):
            own[n, :, cols] = value

        with jax.named_scope(f"keep#g={g}"):
            gate_up_rows(g, 0, last)
            project(g, 0, store)

    def summed(g, n, h):
        arrived(to_partner(g, h), f"partner#g={g}")
        return own[n, parts[h], :] + drecv[g, parts[h], :].astype(f32)

    e_x = remote(esend.at[0], erecv.at[0], e_ss.at[0], e_rs.at[0], to_x)
    e_z = remote(esend.at[1], erecv.at[1], e_ss.at[1], e_rs.at[1], to_z[1])

    def out_copy(n, h, dev):
        return remote(
            ssend.at[n, parts[h]], srecv.at[n, parts[h]], s_ss.at[n, h], s_rs.at[n, h], dev
        )

    out_x, out_z = out_copy(0, 0, to_x), [out_copy(1, h, to_z[1]) for h in range(2)]
    eighth = quarter // 2
    ends = [slice(quarter + n * eighth, quarter + (n + 1) * eighth) for n in range(2)]
    out_end = [
        remote(ssend.at[0, rows_], srecv.at[0, rows_], s_ss.at[0, 1 + n], s_rs.at[0, 1 + n], to_x)
        for n, rows_ in enumerate(ends)
    ]

    send_partner(3, (0, 1))
    keep(3, 2)
    for h, copy in enumerate((e_x, e_z)):
        esend[h] = summed(3, 2, h).astype(bf16)
        start(copy)
    send_partner(1, (0, 1))
    keep(1, 1)
    ssend[0, parts[0], :] = summed(1, 1, 0).astype(bf16)
    start(out_x)
    send_partner(2, (1, 0))
    keep(2, 0)
    ssend[1, parts[1], :] = summed(2, 0, 1).astype(bf16)
    start(out_z[1])
    send_partner(0, (0, 1))

    def add_mixed(cols, value):
        mixed[:, cols] = mixed[:, cols] + value

    gate_up_rows(0, 0, last)
    project(0, 0, add_mixed)
    own[1, parts[1], :] = summed(1, 1, 1)
    own[0, parts[0], :] = summed(2, 0, 0)
    for h in range(2):
        arrived(to_partner(0, h), "partner0")
    mixed[...] = mixed[...] + drecv[0].astype(f32)

    def pass_on(along_x):
        if along_x:
            arrived(e_z, "e_z")
            for n, copy in enumerate(out_end):
                got = erecv[1, n * eighth : (n + 1) * eighth, :].astype(f32)
                ssend[0, ends[n], :] = (own[1, ends[n], :] + got).astype(bf16)
                copy.start()
        else:
            arrived(e_x, "e_x")
            ssend[1, parts[0], :] = (own[0, parts[0], :] + erecv[0].astype(f32)).astype(bf16)
            out_z[0].start()

    by_plane(pass_on, [(True,), (False,)], [(False,), (True,)])
    sent.extend((*out_end, out_z[0]))
    arrived(out_x, "out_x")
    mixed[parts[0], :] = mixed[parts[0], :] + srecv[0, parts[0], :].astype(f32)
    arrived(out_z[1], "out_z1")
    mixed[parts[1], :] = mixed[parts[1], :] + srecv[1, parts[1], :].astype(f32)

    def finish(rows_, n):
        o_ref[rows_, :] = (mixed[rows_, :] + srecv[n, rows_, :].astype(f32)).astype(bf16)

    arrived(out_z[0], "out_z0")
    finish(parts[0], 1)
    for n, copy in enumerate(out_end):
        arrived(copy, "out_end")
        finish(ends[n], 0)

    for copy in [*sent, *copies.values(), *to_y_copies.values()]:
        copy.wait_send()

    @pl.when(sp < sp_count - 1)
    def _():
        for copy in halo(0, (sp + 1, c)):
            copy.wait_send()

    @pl.when(sp > 0)
    def _():
        for copy in halo(1, (sp - 1, c)):
            copy.wait_send()


def fused_shards(
    queries, key_rows, values, sink_logit, residual_in, out_weight, norm_gain,
    gate_weight, up_weight, down_weight,
):
    bf16, f32 = jnp.bfloat16, jnp.float32
    rows, depth = queries.shape[0], residual_in.shape[1]
    half = residual_in.shape[0]
    blocks = lax.axis_size("sp")
    kv = key_rows.shape[1]
    kv_here = kv // HEAD_DIM
    width = down_weight.shape[1]
    units = down_weight.shape[0] // 4
    count = len(chunks_of(units))
    smem = pl.BlockSpec(memory_space=pltpu.SMEM)
    hbm = pl.BlockSpec(memory_space=pl.ANY)
    dma = pltpu.SemaphoreType.DMA
    scratch = [
        pltpu.VMEM(key_rows.shape, bf16),
        pltpu.VMEM(values.shape, bf16),
        pltpu.VMEM((1, depth), f32),
        pltpu.VMEM(gate_weight.shape, bf16),
        pltpu.VMEM(up_weight.shape, bf16),
        pltpu.VMEM((3, down_weight.shape[0], width), bf16),
        pltpu.VMEM(queries.shape, bf16),
        pltpu.VMEM((2, WINDOW, kv), bf16),
        pltpu.VMEM((2, WINDOW, kv), bf16),
        pltpu.VMEM((kv_here, 2, rows + 2 * WINDOW, LANES), bf16),
        pltpu.VMEM((kv_here, 2, rows + 2 * WINDOW, LANES), bf16),
        pltpu.VMEM(queries.shape, bf16),
        pltpu.VMEM(out_weight.shape, bf16),
        pltpu.VMEM((half, depth), bf16),
        pltpu.VMEM((half, depth), bf16),
        pltpu.VMEM((half, depth), f32),
        pltpu.VMEM((4, 2, half, depth), bf16),
        pltpu.VMEM((blocks, 3, units, width), bf16),
        pltpu.VMEM((3, units, width), bf16),
        pltpu.VMEM((4, 2, half, units), bf16),
        pltpu.VMEM((4, half, depth), bf16),
        pltpu.VMEM((4, half, depth), bf16),
        pltpu.VMEM((3, half, depth), f32),
        pltpu.VMEM((2, half // 2, depth), bf16),
        pltpu.VMEM((2, half // 2, depth), bf16),
        pltpu.VMEM((2, half, depth), bf16),
        pltpu.VMEM((2, half, depth), bf16),
        dma((12,)), dma((4,)), dma((4,)), dma((1,)), dma((1,)),
        dma((16, count)), dma((16, count)), dma((count,)), dma((count,)),
        dma((9,)), dma((9,)), dma((4, 2)), dma((4, 2)), dma((2,)), dma((2,)),
        dma((2, 3)), dma((2, 3)),
    ]
    return pl.pallas_call(
        fused,
        out_shape=pltpu.VMEM(residual_in.shape, bf16),
        in_specs=[hbm, hbm, hbm, smem, hbm, hbm, hbm, hbm, hbm, hbm],
        out_specs=pl.BlockSpec(memory_space=pltpu.VMEM),
        scratch_shapes=scratch,
        compiler_params=pltpu.CompilerParams(
            collective_id=0, has_side_effects=True, vmem_limit_bytes=60 * 1024 * 1024
        ),
    )(
        queries, key_rows, values, sink_logit, residual_in, out_weight,
        norm_gain.reshape(1, depth), gate_weight, up_weight, down_weight,
    )


def solution(mesh):
    sp_count, tp_count = mesh.shape["sp"], mesh.shape["tp"]
    group = math.gcd(sp_count, 4)
    if tp_count == 2 and sp_count == 4 * group:
        return jax.shard_map(
            fused_shards,
            mesh=mesh,
            in_specs=(
                P("sp", "tp"),
                P("sp", "tp"),
                P("sp", "tp"),
                P("tp"),
                P(("sp", "tp"), None),
                P("tp", None),
                P(),
                P("sp", "tp"),
                P("sp", "tp"),
                P("tp", "sp"),
            ),
            out_specs=P(("sp", "tp"), None),
            check_vma=False,
        )
    fine = Mesh(mesh.devices.reshape(sp_count // group, group, tp_count), ("o", "q", "tp"))
    sp = ("o", "q")
    return jax.shard_map(
        shards,
        mesh=fine,
        in_specs=(
            P(sp, "tp"),
            P(sp, "tp"),
            P(sp, "tp"),
            P("tp"),
            P(("o", "q", "tp"), None),
            P("tp", None),
            P(),
            P(sp, "tp"),
            P(sp, "tp"),
            P("tp", sp),
        ),
        out_specs=P(("o", "q", "tp"), None),
        check_vma=False,
    )
```
